512 devices in a mesh: kv: 16 (over y, x), tp: 32 (over z, core).
Axes of the slice: x: 4, y: 4, z: 16, core: 2. Of those that a mesh axis runs over, the one named last changes fastest.
Arguments:
- residual: bfloat16 [512, 4096], P(None, ('kv', 'tp')), may hold values from -20 to 20
- mixer_gain: float32 [4096], P('kv'), may hold values from 0.1 to 1.9
- w_query: bfloat16 [4096, 4096], P('kv', 'tp'), may hold values from -0.09375 to 0.09375
- w_forget: bfloat16 [4096, 4096], P('kv', 'tp'), may hold values from -0.09375 to 0.09375
- w_input: bfloat16 [4096, 4096], P('kv', 'tp'), may hold values from -0.09375 to 0.09375
- w_outgate: bfloat16 [4096, 4096], P('kv', 'tp'), may hold values from -0.09375 to 0.09375
- lower_bound: float32 [4096], P('tp'), may hold values from 0.3 to 0.97
- state: float32 [512, 32, 128, 128], P('kv', 'tp'), may hold values from -6 to 6
- head_gain: float32 [128], replicated, may hold values from 0.1 to 1.9
- w_mix_out: bfloat16 [4096, 4096], P('tp', 'kv'), may hold values from -0.09375 to 0.09375
- ffn_gain: float32 [4096], P('kv'), may hold values from 0.1 to 1.9
- w_gate: bfloat16 [4096, 10752], P('kv', 'tp'), may hold values from -0.09375 to 0.09375
- w_up: bfloat16 [4096, 10752], P('kv', 'tp'), may hold values from -0.09375 to 0.09375
- w_down: bfloat16 [10752, 4096], P('tp', 'kv'), may hold values from -0.0625 to 0.0625
Outputs:
- layer_out: bfloat16 [512, 4096], P(None, ('kv', 'tp'))
- new_state: float32 [512, 32, 128, 128], P('kv', 'tp')
The draws below stay inside these ranges and needn't reach their ends.
All inputs are finite; a program needn't handle non-finite values.
Results may differ from the reference program's by a relative error of at most 0.015.
Values may be sent and summed in bfloat16 or wider, within the bound.
A program may use at most 64 MiB of HBM per device.

```python
import jax
import jax.numpy as jnp
from jax import lax

D = 4096
HEADS = 32
DK = 128
DV = 128
FF = 10752
SEQS = 512
HID = 4096
VID = 4096
N_KV = 16
N_TP = 32


def draw_residual(key, part):
    first = jax.random.fold_in(jax.random.fold_in(key, 11), 0)
    column = jnp.arange(D)
    kv_index = (column // (D // N_KV)).astype(jnp.float32)
    tp_index = (column // (D // (N_KV * N_TP)) % N_TP).astype(jnp.float32)
    col_scale = 0.4 * 3.0 ** (kv_index / max(N_KV - 1, 1)) * 3.0 ** (tp_index / max(N_TP - 1, 1))
    values = jnp.clip(jax.random.normal(first, (SEQS, D), jnp.float32), -4.0, 4.0)
    return jnp.clip(values * col_scale, -20.0, 20.0).astype(jnp.bfloat16)


def block_scale(stream_key, extent, pieces, smallest, high):
    gain = 1.0
    for position, shards_of in pieces:
        heights = jax.random.uniform(jax.random.fold_in(jax.random.fold_in(stream_key, 6), position), (shards_of,), jnp.float32, smallest / len(pieces), high / len(pieces))
        gain = gain * jnp.repeat(jnp.exp(heights), extent[position] // shards_of).reshape((-1,) + (1,) * (len(extent) - 1 - position))
    return gain


def scatter_about(stream_key, dims, scale, most, cuts=(), held_as=jnp.bfloat16):
    drawn = scale * jax.random.normal(stream_key, dims, jnp.float32)
    if cuts:
        drawn = drawn * block_scale(stream_key, dims, cuts, -0.22, 0.18)
    return jnp.clip(drawn, -most, most).astype(held_as)


def setup_inputs(seed: int = 0) -> dict:
    key_of = jax.random.split(jax.random.key(seed), 15)
    return {
        "residual": draw_residual(jax.random.fold_in(key_of[14], 71), 0),
        "mixer_gain": jnp.clip(1.0 + 0.18 * jax.random.normal(key_of[1], (D,), jnp.float32), 0.1, 1.9),
        "w_query": scatter_about(key_of[2], (D, HID), D ** -0.5, 0.09375, ((0, 16), (1, 32))),
        "w_forget": scatter_about(key_of[3], (D, HID), D ** -0.5, 0.09375, ((0, 16), (1, 32))),
        "w_input": scatter_about(key_of[4], (D, VID), D ** -0.5, 0.09375, ((0, 16), (1, 32))),
        "w_outgate": scatter_about(key_of[5], (D, VID), D ** -0.5, 0.09375, ((0, 16), (1, 32))),
        "lower_bound": jnp.clip(0.3 + 0.67 * jax.random.uniform(key_of[6], (HID,), jnp.float32) ** block_scale(key_of[6], (HID,), ((0, 32),), -0.2, 0.2), 0.3, 0.97),
        "state": scatter_about(key_of[7], (SEQS, HEADS, DK, DV), 1.0, 6.0, ((0, 16), (1, 32)), jnp.float32),
        "head_gain": jnp.clip(1.0 + 0.18 * jax.random.normal(key_of[8], (DV,), jnp.float32), 0.1, 1.9),
        "w_mix_out": scatter_about(key_of[9], (VID, D), VID ** -0.5, 0.09375, ((0, 32), (1, 16))),
        "ffn_gain": jnp.clip(1.0 + 0.18 * jax.random.normal(key_of[10], (D,), jnp.float32), 0.1, 1.9),
        "w_gate": scatter_about(key_of[11], (D, FF), D ** -0.5, 0.09375, ((0, 16), (1, 32))),
        "w_up": scatter_about(key_of[12], (D, FF), D ** -0.5, 0.09375, ((0, 16), (1, 32))),
        "w_down": scatter_about(key_of[13], (FF, D), FF ** -0.5, 0.0625, ((0, 32), (1, 16))),
    }


EPS = 1e-06

def reference(residual, mixer_gain, w_query, w_forget, w_input, w_outgate, lower_bound, state, head_gain, w_mix_out, ffn_gain, w_gate, w_up, w_down):
    seqs = residual.shape[0]
    xf = residual.astype(jnp.float32)
    inv_a = lax.rsqrt(lax.optimization_barrier(jnp.mean(xf * xf, axis=1, keepdims=True)) + EPS)
    scaled_a = (xf * mixer_gain).astype(jnp.bfloat16)
    query_raw = inv_a * jnp.dot(scaled_a, w_query, preferred_element_type=jnp.float32)
    forget_raw = inv_a * jnp.dot(scaled_a, w_forget, preferred_element_type=jnp.float32)
    value_raw = inv_a * jnp.dot(scaled_a, w_input, preferred_element_type=jnp.float32)
    outgate_raw = inv_a * jnp.dot(scaled_a, w_outgate, preferred_element_type=jnp.float32)
    bound = lower_bound.reshape(HEADS, DK)
    forget_raw = forget_raw.reshape(seqs, HEADS, DK)
    forget = bound + (1.0 - bound) * jax.nn.sigmoid(forget_raw)
    keyvec = (1.0 - bound) * jax.nn.sigmoid(-forget_raw)
    query = jax.nn.silu(query_raw.reshape(seqs, HEADS, DK))
    values = value_raw.reshape(seqs, HEADS, DV)
    new_state = forget[..., None] * state + keyvec[..., None] * values[:, :, None, :]
    head_out = jnp.einsum('shc,shce->she', query, new_state, precision=lax.Precision.HIGHEST)
    inv_h = lax.rsqrt(lax.optimization_barrier(jnp.mean(head_out * head_out, axis=2, keepdims=True)) + EPS)
    normed = head_out * inv_h * head_gain * jax.nn.silu(outgate_raw.reshape(seqs, HEADS, DV))
    normed = normed.reshape(seqs, HEADS * DV).astype(jnp.bfloat16)
    after_mix = (xf + jnp.dot(normed, w_mix_out, preferred_element_type=jnp.float32)).astype(jnp.bfloat16)
    af = after_mix.astype(jnp.float32)
    inv_b = lax.rsqrt(lax.optimization_barrier(jnp.mean(af * af, axis=1, keepdims=True)) + EPS)
    scaled_b = (af * ffn_gain).astype(jnp.bfloat16)
    gate = inv_b * jnp.dot(scaled_b, w_gate, preferred_element_type=jnp.float32)
    upper = inv_b * jnp.dot(scaled_b, w_up, preferred_element_type=jnp.float32)
    hidden = (jax.nn.silu(gate) * upper).astype(jnp.bfloat16)
    layer_out = (af + jnp.dot(hidden, w_down, preferred_element_type=jnp.float32)).astype(jnp.bfloat16)
    return (layer_out, new_state)
```

```python
import functools

import jax
import jax.numpy as jnp
from jax import lax
from jax.experimental import pallas as pl
from jax.experimental.pallas import tpu as pltpu
from jax.sharding import PartitionSpec as P

D = 4096
EPS = 1e-06
KV = 16
Z = 16
SEQ = 512
LOC = 32
F = 256
FFL = 336
FFP = 384
MESH = pl.DeviceIdType.MESH
NT = (((1,), (1,)), ((), ()))
f32 = jnp.float32
bf16 = jnp.bfloat16


def sigmoid(u):
    return 1.0 / (1.0 + jnp.exp(-u))


def silu(u):
    return u * sigmoid(u)


def z_step(j):
    sign = 1 - 2 * lax.rem(j, 2)
    return 8 + sign * ((j + 1) // 2)


def layer_kernel(
    x_ref, mg_ref, lb_ref, hg_ref, fg_ref,
    wq_hbm, wf_hbm, wi_hbm, wo_hbm, state_hbm, wm_hbm, wg_hbm, wu_hbm, wd_hbm,
    out_ref, ns_hbm,
    wp, wm, wg, wu, wd, st, ns,
    x1, s2, sq2, r2, rq2, qt, ft, kt, vals, ho, n3, t4, p4, d4, s4, r4, own5, x5,
    s6, r6, h7, hw7, t8, p8, d8, s8, r8,
    wsem, stsem, nssem, loc,
    s1s, r1s, f1s, f1r, s2s, r2s, q2s, q2r, s3s, r3s, d4s, d4r, s4s, r4s,
    s5s, r5s, f5s, f5r, s6s, r6s, s7s, r7s, d8s, d8r, s8s, r8s,
):
    k = lax.axis_index("kv")
    t = lax.axis_index("tp")
    z = t // 2
    c = lax.rem(t, 2)
    o = 1 - c
    ky = k // 4
    kx = lax.rem(k, 4)
    mate = 2 * z + o

    def kv_to(r):
        return lax.rem(ky + r // 4, 4) * 4 + lax.rem(kx + lax.rem(r, 4), 4)

    def z_to(r):
        return lax.rem(z + r, Z)

    def z_from(r):
        return lax.rem(z - r + Z, Z)

    def rcopy(src, dst, ssem, rsem, kk, tt):
        return pltpu.make_async_remote_copy(
            src_ref=src, dst_ref=dst, send_sem=ssem, recv_sem=rsem,
            device_id=(kk, tt), device_id_type=MESH,
        )

    def all_sent(view, ssem, rsem):
        rcopy(view, view, ssem, rsem, k, mate).wait_send()

    def all_here(view, ssem, rsem):
        rcopy(view, view, ssem, rsem, k, mate).wait_recv()

    loads = [
        pltpu.make_async_copy(src, dst, wsem.at[i])
        for i, (src, dst) in enumerate(
            (
                (wq_hbm, wp.at[0]), (wf_hbm, wp.at[1]), (wi_hbm, wp.at[2]), (wo_hbm, wp.at[3]),
                (wm_hbm, wm), (wg_hbm, wg), (wu_hbm, wu), (wd_hbm, wd),
            )
        )
    ]
    for load in loads:
        load.start()
    state_in = pltpu.make_async_copy(state_hbm, st, stsem)
    state_in.start()

    barrier = pltpu.get_barrier_semaphore()

    def greet_z(j, _):
        pl.semaphore_signal(barrier, inc=1, device_id=(k, 2 * z_to(z_step(j)) + c), device_id_type=MESH)
        return 0

    def greet_kv(r, _):
        pl.semaphore_signal(barrier, inc=1, device_id=(kv_to(r), t), device_id_type=MESH)
        return 0

    lax.fori_loop(0, Z - 1, greet_z, 0)
    lax.fori_loop(1, KV, greet_kv, 0)
    pl.semaphore_signal(barrier, inc=1, device_id=(k, mate), device_id_type=MESH)
    pl.semaphore_wait(barrier, (Z - 1) + (KV - 1) + 1)

    def gather_tp(own, slots, ss, rs, fs, fr):
        def send(j, _):
            r = z_step(j)
            rcopy(own, slots.at[t], ss, rs.at[r], k, 2 * z_to(r) + c).start()
            return 0

        lax.fori_loop(0, Z - 1, send, 0)
        rcopy(own, slots.at[t], fs, fr, k, mate).start()

        def forward(i, _):
            r = z_step(Z - 2 - i)
            src = 2 * z_from(r) + c
            rcopy(own, slots.at[src], ss, rs.at[r], k, mate).wait_recv()
            rcopy(slots.at[src], slots.at[src], fs, fr, k, mate).start()
            return 0

        lax.fori_loop(0, Z - 1, forward, 0)
        all_here(slots.at[pl.ds(0, Z)], fs, fr)

    x1[t] = x_ref[...]
    gather_tp(x_ref, x1, s1s, r1s, f1s, f1r)

    xt = x1[...].astype(f32).reshape(F, SEQ)
    row = jnp.sum(xt * xt, axis=0, keepdims=True)
    for i in range(4):
        sq2[i : i + 1, :] = row[:, 128 * i : 128 * i + 128]
        sq2[4 + i : 5 + i, :] = row[:, 128 * i : 128 * i + 128]
    xf = xt.T
    scaled = (xf * mg_ref[...]).astype(bf16)
    for i in range(4):
        loads[i].wait()
        part = jnp.dot(scaled, wp[i], preferred_element_type=f32)
        s2[:, :, 128 * i : 128 * i + 128] = part.astype(bf16).reshape(KV, LOC, 128)

    def send2(r, _):
        kk = kv_to(r)
        rcopy(s2.at[kk], r2.at[r - 1], s2s, r2s, kk, t).start()
        rcopy(sq2, rq2.at[r - 1], q2s, q2r, kk, t).start()
        return 0

    lax.fori_loop(1, KV, send2, 0)
    state_in.wait()
    all_here(rq2, q2s, q2r)
    all_here(r2, s2s, r2s)

    sq = sq2[...]
    raw = s2[k].astype(f32)
    for i in range(KV - 1):
        sq = sq + rq2[i]
        raw = raw + r2[i].astype(f32)
    tile_row = lax.broadcasted_iota(jnp.int32, (8, 128), 0)
    line = jnp.sum(jnp.where(tile_row == ky, sq, 0.0), axis=0, keepdims=True)
    lane = lax.broadcasted_iota(jnp.int32, (LOC, 128), 1)
    seq = lax.broadcasted_iota(jnp.int32, (LOC, 128), 0)
    total = jnp.sum(jnp.where(lane == seq + kx * LOC, line, 0.0), axis=1, keepdims=True)
    raw = raw * lax.rsqrt(total / D + EPS)

    bound = lb_ref[...]
    forget_raw = raw[:, 128:256]
    forget = bound + (1.0 - bound) * sigmoid(forget_raw)
    keyvec = (1.0 - bound) * sigmoid(-forget_raw)
    query = silu(raw[:, 0:128])
    vals[...] = raw[:, 256:384]
    out_gate = silu(raw[:, 384:512])
    fill = jnp.zeros((128 - LOC, 128), f32)
    qt[...] = jnp.concatenate([query, fill], axis=0).T
    ft[...] = jnp.concatenate([forget, fill], axis=0).T
    kt[...] = jnp.concatenate([keyvec, fill], axis=0).T
    lanes = lax.broadcasted_iota(jnp.int32, (128, 128), 1)

    def recur(s, _):
        here = lanes == s

        def column(ref):
            return jnp.sum(jnp.where(here, ref[...], 0.0), axis=1, keepdims=True)

        new = column(ft) * st[s] + column(kt) * vals[pl.ds(s, 1), :]
        ns[s] = new
        ho[pl.ds(s, 1), :] = jnp.sum(column(qt) * new, axis=0, keepdims=True)
        return 0

    lax.fori_loop(0, LOC, recur, 0)
    state_out = pltpu.make_async_copy(ns, ns_hbm, nssem)
    state_out.start()

    head = ho[...]
    inv = lax.rsqrt(jnp.mean(head * head, axis=1, keepdims=True) + EPS)
    own3 = (head * inv * hg_ref[...] * out_gate).astype(bf16)

    n3[k] = own3

    def send3(r, _):
        rcopy(n3.at[k], n3.at[k], s3s, r3s, kv_to(r), t).start()
        return 0

    lax.fori_loop(1, KV, send3, 0)
    loads[4].wait()
    all_here(n3.at[pl.ds(0, KV - 1)], s3s, r3s)

    mixed = jnp.dot(n3[...].reshape(SEQ, 128), wm[...], preferred_element_type=f32)
    for b in range(2 * Z):
        t4[b % 2, b // 2] = mixed[16 * b : 16 * b + 16, :]

    def sum_tp(terms, pairs, got, ring, land, ds_, dr_, ss, rs):
        pairs[...] = terms[o].astype(bf16)
        swap = rcopy(pairs, got, ds_, dr_, k, mate)
        swap.start()
        swap.wait_recv()
        both = terms[c] + got[...].astype(f32)
        ring[...] = both.astype(bf16)
        terms[c] = both

        def send(j, _):
            r = z_step(j)
            zz = z_to(r)
            rcopy(ring.at[zz], land.at[r - 1], ss, rs, k, 2 * zz + c).start()
            return 0

        lax.fori_loop(0, Z - 1, send, 0)
        all_here(land, ss, rs)
        total_ = terms[c, z]
        for i in range(Z - 1):
            total_ = total_ + land[i].astype(f32)
        return total_

    summed = sum_tp(t4, p4, d4, s4, r4, d4s, d4r, s4s, r4s)
    hw7[...] = xf
    mine = hw7[pl.ds(pl.multiple_of(t * 16, 16), 16), :]
    own5[...] = (mine + summed).astype(bf16)
    x5[t] = own5[...]
    gather_tp(own5, x5, s5s, r5s, f5s, f5r)

    after = x5[...].reshape(SEQ, F).astype(f32)
    squares = jnp.sum(after * after, axis=1, keepdims=True)
    scaled = (after * fg_ref[...]).astype(bf16)
    loads[5].wait()
    gate = lax.dot_general(scaled, wg[...], NT, preferred_element_type=f32)
    s6[:, :, 0:FFL] = gate.astype(bf16).reshape(KV, LOC, FFL)
    loads[6].wait()
    upper = lax.dot_general(scaled, wu[...], NT, preferred_element_type=f32)
    s6[:, :, FFP : FFP + FFL] = upper.astype(bf16).reshape(KV, LOC, FFL)
    high = squares.astype(bf16)
    low = (squares - high.astype(f32)).astype(bf16)
    spot = lax.broadcasted_iota(jnp.int32, (SEQ, FFP - FFL), 1)
    tail = jnp.where(spot == 0, high.astype(f32), jnp.where(spot == 1, low.astype(f32), 0.0))
    s6[:, :, FFL:FFP] = tail.astype(bf16).reshape(KV, LOC, FFP - FFL)
    s6[:, :, FFP + FFL : 2 * FFP] = jnp.zeros((KV, LOC, FFP - FFL), bf16)

    def send6(r, _):
        kk = kv_to(r)
        rcopy(s6.at[kk], r6.at[r - 1], s6s, r6s, kk, t).start()
        return 0

    lax.fori_loop(1, KV, send6, 0)
    hw7[...] = after
    own_t = hw7[...].T
    loads[7].wait()
    all_here(r6, s6s, r6s)
    both = s6[k].astype(f32)
    for i in range(KV - 1):
        both = both + r6[i].astype(f32)
    total = both[:, FFL : FFL + 1] + both[:, FFL + 1 : FFL + 2]
    inverse = lax.rsqrt(total / D + EPS)
    hidden = silu(both[:, 0:FFP] * inverse) * (both[:, FFP : 2 * FFP] * inverse)
    spot = lax.broadcasted_iota(jnp.int32, (LOC, FFP), 1)
    h7[k] = jnp.where(spot < FFL, hidden, 0.0).astype(bf16)

    def send7(r, _):
        rcopy(h7.at[k], h7.at[k], s7s, r7s, kv_to(r), t).start()
        return 0

    lax.fori_loop(1, KV, send7, 0)
    t8[...] = own_t.reshape(2 * Z, 8, SEQ)
    own8 = t8[t]
    all_here(h7.at[pl.ds(0, KV - 1)], s7s, r7s)
    hall = h7[...].reshape(SEQ, FFP)
    down = jnp.dot(hall[:, 0:FFL], wd[...], preferred_element_type=f32)
    down = down.T
    for b in range(2 * Z):
        p = down[8 * b : 8 * b + 8, :]
        d = b
        t8[(d % 2) * Z + d // 2] = p

    summed = sum_tp8(t8, p8, d8, s8, r8, d8s, d8r, s8s, r8s, c, o, z, k, mate, rcopy, all_here, z_to)
    out_ref[...] = (own8 + summed).astype(bf16)

    slots = x1.at[pl.ds(0, Z - 1)]
    all_sent(slots, s1s, r1s.at[0])
    all_sent(x1.at[pl.ds(0, Z)], f1s, f1r)
    all_sent(r2, s2s, r2s)
    all_sent(rq2, q2s, q2r)
    all_sent(n3.at[pl.ds(0, KV - 1)], s3s, r3s)
    all_sent(p4, d4s, d4r)
    all_sent(r4, s4s, r4s)
    all_sent(x5.at[pl.ds(0, Z - 1)], s5s, r5s.at[0])
    all_sent(x5.at[pl.ds(0, Z)], f5s, f5r)
    all_sent(r6, s6s, r6s)
    all_sent(h7.at[pl.ds(0, KV - 1)], s7s, r7s)
    all_sent(p8, d8s, d8r)
    all_sent(r8, s8s, r8s)
    state_out.wait()


def sum_tp8(terms, pairs, got, ring, land, ds_, dr_, ss, rs, c, o, z, k, mate, rcopy, all_here, z_to):
    pairs[...] = terms[pl.ds(o * Z, Z)].astype(bf16)
    swap = rcopy(pairs, got, ds_, dr_, k, mate)
    swap.start()
    swap.wait_recv()
    both = terms[pl.ds(c * Z, Z)] + got[...].astype(f32)
    ring[...] = both.astype(bf16)
    terms[pl.ds(c * Z, Z)] = both

    def send(j, _):
        r = z_step(j)
        zz = z_to(r)
        rcopy(ring.at[zz], land.at[r - 1], ss, rs, k, 2 * zz + c).start()
        return 0

    lax.fori_loop(0, Z - 1, send, 0)
    all_here(land, ss, rs)
    total = terms[c * Z + z]
    for i in range(Z - 1):
        total = total + land[i].astype(f32)
    return total


def body(
    residual, mixer_gain, w_query, w_forget, w_input, w_outgate, lower_bound, state, head_gain,
    w_mix_out, ffn_gain, w_gate, w_up, w_down,
):
    vmem = pl.BlockSpec(memory_space=pltpu.VMEM)
    hbm = pl.BlockSpec(memory_space=pl.ANY)
    V = pltpu.VMEM
    dma = pltpu.SemaphoreType.DMA
    scratch = [
        V((4, F, 128), bf16), V((128, F), bf16), V((FFL, F), bf16), V((FFL, F), bf16), V((FFL, F), bf16),
        V((LOC, 128, 128), f32), V((LOC, 128, 128), f32),
        V((2 * Z, 8, SEQ), bf16),
        V((KV, LOC, 512), bf16), V((8, 128), f32), V((KV - 1, LOC, 512), bf16), V((KV - 1, 8, 128), f32),
        V((128, 128), f32), V((128, 128), f32), V((128, 128), f32), V((LOC, 128), f32), V((LOC, 128), f32),
        V((KV, LOC, 128), bf16),
        V((2, Z, 16, F), f32), V((Z, 16, F), bf16), V((Z, 16, F), bf16), V((Z, 16, F), bf16), V((Z - 1, 16, F), bf16),
        V((16, F), bf16), V((2 * Z, 16, F), bf16),
        V((KV, LOC, 2 * FFP), bf16), V((KV - 1, LOC, 2 * FFP), bf16), V((KV, LOC, FFP), bf16), V((SEQ, F), f32),
        V((2 * Z, 8, SEQ), f32), V((Z, 8, SEQ), bf16), V((Z, 8, SEQ), bf16), V((Z, 8, SEQ), bf16), V((Z - 1, 8, SEQ), bf16),
        dma((8,)), dma, dma, dma,
        dma, dma((Z,)), dma, dma, dma, dma, dma, dma, dma, dma, dma, dma, dma, dma,
        dma, dma((Z,)), dma, dma, dma, dma, dma, dma, dma, dma, dma, dma,
    ]
    out, new_state = pl.pallas_call(
        layer_kernel,
        out_shape=(
            jax.ShapeDtypeStruct((8, SEQ), bf16),
            jax.ShapeDtypeStruct((LOC, 128, 128), f32),
        ),
        in_specs=[vmem] * 5 + [hbm] * 9,
        out_specs=(vmem, hbm),
        scratch_shapes=scratch,
        compiler_params=pltpu.CompilerParams(
            collective_id=0, has_side_effects=True, vmem_limit_bytes=56 * 1024 * 1024
        ),
    )(
        residual.T, mixer_gain.reshape(1, F), lower_bound.reshape(1, 128), head_gain.reshape(1, 128),
        ffn_gain.reshape(1, F), w_query, w_forget, w_input, w_outgate, state.reshape(LOC, 128, 128),
        w_mix_out, w_gate.T, w_up.T, w_down,
    )
    return out.T, new_state.reshape(LOC, 1, 128, 128)


def solution(mesh):
    in_specs = (
        P(None, ("kv", "tp")), P("kv"), P("kv", "tp"), P("kv", "tp"), P("kv", "tp"), P("kv", "tp"), P("tp"),
        P("kv", "tp", None, None), P(), P("tp", "kv"), P("kv"), P("kv", "tp"), P("kv", "tp"), P("tp", "kv"),
    )
    out_specs = (P(None, ("kv", "tp")), P("kv", "tp", None, None))
    return jax.shard_map(body, mesh=mesh, in_specs=in_specs, out_specs=out_specs, check_vma=False)
```

```python
import jax
import jax.numpy as jnp
from jax import lax
from jax.experimental import pallas as pl
from jax.experimental.pallas import tpu as pltpu
from jax.sharding import PartitionSpec as P

D = 4096
EPS = 1e-06
N = 4
Z = 16
ROWS = 128
LOC = 32
F = 256
FFL = 336
FFP = 384
MESH = pl.DeviceIdType.MESH
NT = (((1,), (1,)), ((), ()))
f32 = jnp.float32
bf16 = jnp.bfloat16


def sigmoid(u):
    return 1.0 / (1.0 + jnp.exp(-u))


def silu(u):
    return u * sigmoid(u)


def z_step(j):
    sign = 1 - 2 * lax.rem(j, 2)
    return 8 + sign * ((j + 1) // 2)


def layer_kernel(
    x_hbm, mg_hbm, lb_hbm, hg_hbm, fg_hbm,
    wq_hbm, wf_hbm, wi_hbm, wo_hbm, state_hbm, wm_hbm, wg_hbm, wu_hbm, wd_hbm,
    out_ref, ns,
    x_ref, mg_ref, lb_ref, hg_ref, fg_ref, wp, wm, wg, wu, wd, gains, st,
    xa, x1, xf, s2, sq2, r2, rq2, qfk, vals, ho, n3, t4, p4, d4, s4, r4, own5, x5, xt5,
    s6, r6, h7, t8, p8, d8, s8, r8, o9,
    wsem, stsem, wps, wpr, wms, wmr, wgs, wgr, wus, wur, wds, wdr, gs, gr, s0s, r0s,
    s1s, r1s, f1s, f1r, s2s, r2s, q2s, q2r, s3s, r3s, d4s, d4r, s4s, r4s,
    s5s, r5s, f5s, f5r, s6s, r6s, s7s, r7s, d8s, d8r, s8s, r8s, s9s, r9s,
):
    k = lax.axis_index("kv")
    t = lax.axis_index("tp")
    z = t // 2
    c = lax.rem(t, 2)
    o = 1 - c
    y = k // N
    x = lax.rem(k, N)
    mate = 2 * z + o

    def turn(a, r):
        return lax.rem(a + r, N)

    def y_to(r):
        return turn(y, r) * N + x

    def x_to(r):
        return y * N + turn(x, r)

    def z_to(r):
        return lax.rem(z + r, Z)

    def z_from(r):
        return lax.rem(z - r + Z, Z)

    def rcopy(src, dst, ssem, rsem, kk, tt):
        return pltpu.make_async_remote_copy(
            src_ref=src, dst_ref=dst, send_sem=ssem, recv_sem=rsem,
            device_id=(kk, tt), device_id_type=MESH,
        )

    def all_sent(view, ssem, rsem):
        rcopy(view, view, ssem, rsem, k, mate).wait_send()

    def all_here(view, ssem, rsem):
        rcopy(view, view, ssem, rsem, k, mate).wait_recv()

    def three(ref):
        return ref.at[pl.ds(0, N - 1)]

    def greet(kk, tt):
        barrier = pltpu.get_barrier_semaphore()
        pl.semaphore_signal(barrier, inc=1, device_id=(kk, tt), device_id_type=MESH)

    def greet_z(j, _):
        greet(k, 2 * z_to(z_step(j)) + c)
        return 0

    lax.fori_loop(0, Z - 1, greet_z, 0)
    for r in range(1, N):
        greet(y_to(r), t)
        greet(x_to(r), t)
    greet(k, mate)

    loads = [
        pltpu.make_async_copy(src, dst, wsem.at[i])
        for i, (src, dst) in enumerate(
            (
                (wq_hbm, wp.at[y, 0]), (wf_hbm, wp.at[y, 1]), (wi_hbm, wp.at[y, 2]), (wo_hbm, wp.at[y, 3]),
                (wm_hbm, wm.at[y]), (wg_hbm, wg.at[y]), (wu_hbm, wu.at[y]), (wd_hbm, wd.at[y]),
                (x_hbm, x_ref), (mg_hbm, mg_ref), (lb_hbm, lb_ref), (hg_hbm, hg_ref), (fg_hbm, fg_ref),
            )
        )
    ]
    for load in loads:
        load.start()
    state_in = pltpu.make_async_copy(state_hbm, st, stsem)
    state_in.start()
    for load in loads:
        load.wait()
    gains[y, 0:1, :] = mg_ref[...]
    gains[y, 1:2, :] = fg_ref[...]
    pl.semaphore_wait(pltpu.get_barrier_semaphore(), (Z - 1) + 2 * (N - 1) + 1)

    for r in range(1, N):
        there = turn(y, r)
        lanes = pl.ds(pl.multiple_of(there * ROWS, ROWS), ROWS)
        rcopy(x_ref.at[:, lanes], xa.at[y], s0s, r0s, y_to(r), t).start()
        rcopy(gains.at[y], gains.at[y], gs, gr, y_to(r), t).start()
    for ref, ss, rs in ((wp, wps, wpr), (wm, wms, wmr), (wg, wgs, wgr), (wu, wus, wur), (wd, wds, wdr)):
        for r in range(1, N):
            rcopy(ref.at[y], ref.at[y], ss, rs, y_to(r), t).start()
    mine = pl.ds(pl.multiple_of(y * ROWS, ROWS), ROWS)
    xa[y] = x_ref[:, mine]
    all_here(three(xa), s0s, r0s)

    def gather_tp(own, slots, ss, rs, fs, fr):
        def send(j, _):
            r = z_step(j)
            rcopy(own, slots.at[t], ss, rs.at[r], k, 2 * z_to(r) + c).start()
            return 0

        lax.fori_loop(0, Z - 1, send, 0)
        rcopy(own, slots.at[t], fs, fr, k, mate).start()

        def forward(i, _):
            r = z_step(Z - 2 - i)
            src = 2 * z_from(r) + c
            rcopy(own, slots.at[src], ss, rs.at[r], k, mate).wait_recv()
            rcopy(slots.at[src], slots.at[src], fs, fr, k, mate).start()
            return 0

        lax.fori_loop(0, Z - 1, forward, 0)
        all_here(slots.at[pl.ds(0, Z)], fs, fr)

    x1[t] = xa[...]
    gather_tp(xa, x1, s1s, r1s, f1s, f1r)
    all_here(three(gains), gs, gr)
    all_here(three(wp), wps, wpr)

    row = jnp.zeros((1, ROWS), f32)
    scaled = []
    for b in range(N):
        xt = x1[:, b].astype(f32).reshape(F, ROWS)
        row = row + jnp.sum(xt * xt, axis=0, keepdims=True)
        rows = xt.T
        xf[b] = rows
        scaled.append((rows * gains[b, 0:1, :]).astype(bf16))
    sq2[...] = jnp.broadcast_to(row, (8, ROWS))
    for i in range(4):
        part = jnp.dot(scaled[0], wp[0, i], preferred_element_type=f32)
        for b in range(1, N):
            part = part + jnp.dot(scaled[b], wp[b, i], preferred_element_type=f32)
        s2[:, :, 128 * i : 128 * i + 128] = part.astype(bf16).reshape(N, LOC, 128)

    for r in range(1, N):
        rcopy(s2.at[turn(x, r)], r2.at[r - 1], s2s, r2s, x_to(r), t).start()
        rcopy(sq2, rq2.at[r - 1], q2s, q2r, x_to(r), t).start()
    state_in.wait()
    all_here(rq2, q2s, q2r)
    all_here(r2, s2s, r2s)

    sq = sq2[...]
    raw = s2[x].astype(f32)
    for i in range(N - 1):
        sq = sq + rq2[i]
        raw = raw + r2[i].astype(f32)
    lane = lax.broadcasted_iota(jnp.int32, (LOC, ROWS), 1)
    seq = lax.broadcasted_iota(jnp.int32, (LOC, ROWS), 0)
    total = jnp.sum(jnp.where(lane == seq + x * LOC, sq[0:1, :], 0.0), axis=1, keepdims=True)
    raw = raw * lax.rsqrt(total / D + EPS)

    bound = lb_ref[...]
    forget_raw = raw[:, 128:256]
    forget = bound + (1.0 - bound) * sigmoid(forget_raw)
    keyvec = (1.0 - bound) * sigmoid(-forget_raw)
    query = silu(raw[:, 0:128])
    vals[...] = raw[:, 256:384]
    out_gate = silu(raw[:, 384:512])
    qfk[...] = jnp.concatenate([query, forget, keyvec, jnp.zeros((LOC, 128), f32)], axis=0).T

    for s in range(LOC):
        new = qfk[:, LOC + s : LOC + s + 1] * st[s] + qfk[:, 2 * LOC + s : 2 * LOC + s + 1] * vals[s : s + 1, :]
        ns[s] = new
        ho[s : s + 1, :] = jnp.sum(qfk[:, s : s + 1] * new, axis=0, keepdims=True)

    head = ho[...]
    inv = lax.rsqrt(jnp.mean(head * head, axis=1, keepdims=True) + EPS)
    n3[x] = (head * inv * hg_ref[...] * out_gate).astype(bf16)

    for r in range(1, N):
        rcopy(n3.at[x], n3.at[x], s3s, r3s, x_to(r), t).start()
    all_here(three(wm), wms, wmr)
    all_here(three(n3), s3s, r3s)

    heads = n3[...].reshape(ROWS, 128)
    for b in range(N):
        mixed = jnp.dot(heads, wm[b], preferred_element_type=f32)
        for i in range(8):
            tt = 8 * b + i
            t4[tt % 2, tt // 2] = mixed[16 * i : 16 * i + 16, :]

    def sum_tp(terms, pairs, got, ring, land, ds_, dr_, ss, rs):
        pairs[...] = terms[o].astype(bf16)
        swap = rcopy(pairs, got, ds_, dr_, k, mate)
        swap.start()
        swap.wait_recv()
        both = terms[c] + got[...].astype(f32)
        ring[...] = both.astype(bf16)
        terms[c] = both

        def send(j, _):
            r = z_step(j)
            zz = z_to(r)
            rcopy(ring.at[zz], land.at[r - 1], ss, rs, k, 2 * zz + c).start()
            return 0

        lax.fori_loop(0, Z - 1, send, 0)
        all_here(land, ss, rs)
        result = terms[c, z]
        for i in range(Z - 1):
            result = result + land[i].astype(f32)
        return result

    summed = sum_tp(t4, p4, d4, s4, r4, d4s, d4r, s4s, r4s)
    block = xf[t // 8, pl.ds(pl.multiple_of(lax.rem(t, 8) * 16, 16), 16), :]
    own5[...] = (block + summed).astype(bf16)
    x5[t] = own5[...]
    gather_tp(own5, x5, s5s, r5s, f5s, f5r)
    all_here(three(wg), wgs, wgr)
    all_here(three(wu), wus, wur)

    squares = jnp.zeros((ROWS, 1), f32)
    scaled = []
    for b in range(N):
        after = x5[8 * b : 8 * b + 8].reshape(ROWS, F).astype(f32)
        squares = squares + jnp.sum(after * after, axis=1, keepdims=True)
        scaled.append((after * gains[b, 1:2, :]).astype(bf16))

    def projected(w):
        acc = lax.dot_general(scaled[0], w[0], NT, preferred_element_type=f32)
        for b in range(1, N):
            acc = acc + lax.dot_general(scaled[b], w[b], NT, preferred_element_type=f32)
        return acc.astype(bf16).reshape(N, LOC, FFL)

    s6[:, :, 0:FFL] = projected(wg)
    s6[:, :, FFP : FFP + FFL] = projected(wu)
    high = squares.astype(bf16).astype(f32)
    spot = lax.broadcasted_iota(jnp.int32, (ROWS, FFP - FFL), 1)
    tail = jnp.where(spot == 0, high, jnp.where(spot == 1, squares - high, 0.0))
    s6[:, :, FFL:FFP] = tail.astype(bf16).reshape(N, LOC, FFP - FFL)
    s6[:, :, FFP + FFL : 2 * FFP] = jnp.zeros((N, LOC, FFP - FFL), bf16)

    for r in range(1, N):
        rcopy(s6.at[turn(x, r)], r6.at[r - 1], s6s, r6s, x_to(r), t).start()
    for b in range(N):
        xt5[b] = x5[8 * b : 8 * b + 8].reshape(ROWS, F).astype(f32).T.reshape(2 * Z, 8, ROWS)
    all_here(r6, s6s, r6s)
    both = s6[x].astype(f32)
    for i in range(N - 1):
        both = both + r6[i].astype(f32)
    total = both[:, FFL : FFL + 1] + both[:, FFL + 1 : FFL + 2]
    inverse = lax.rsqrt(total / D + EPS)
    hidden = silu(both[:, 0:FFP] * inverse) * (both[:, FFP : 2 * FFP] * inverse)
    spot = lax.broadcasted_iota(jnp.int32, (LOC, FFP), 1)
    h7[x] = jnp.where(spot < FFL, hidden, 0.0).astype(bf16)

    for r in range(1, N):
        rcopy(h7.at[x], h7.at[x], s7s, r7s, x_to(r), t).start()
    all_here(three(wd), wds, wdr)
    all_here(three(h7), s7s, r7s)
    hall = h7[...].reshape(ROWS, FFP)[:, 0:FFL]
    for b in range(N):
        down = jnp.dot(hall, wd[b], preferred_element_type=f32).T
        for i in range(2 * Z):
            t8[i % 2, i // 2, b] = down[8 * i : 8 * i + 8, :]

    summed = sum_tp(t8, p8, d8, s8, r8, d8s, d8r, s8s, r8s)
    o9[...] = (xt5[:, t] + summed).astype(bf16)
    for r in range(1, N):
        rcopy(o9.at[turn(y, r)], out_ref.at[:, mine], s9s, r9s, y_to(r), t).start()
    out_ref[:, mine] = o9[y]
    three_out = out_ref.at[:, pl.ds(0, (N - 1) * ROWS)]
    all_here(three_out, s9s, r9s)

    all_sent(three(xa), s0s, r0s)
    all_sent(three(gains), gs, gr)
    for ref, ss, rs in ((wp, wps, wpr), (wm, wms, wmr), (wg, wgs, wgr), (wu, wus, wur), (wd, wds, wdr)):
        all_sent(three(ref), ss, rs)
    all_sent(x1.at[pl.ds(0, Z - 1)], s1s, r1s.at[0])
    all_sent(x1.at[pl.ds(0, Z)], f1s, f1r)
    all_sent(r2, s2s, r2s)
    all_sent(rq2, q2s, q2r)
    all_sent(three(n3), s3s, r3s)
    all_sent(p4, d4s, d4r)
    all_sent(r4, s4s, r4s)
    all_sent(x5.at[pl.ds(0, Z - 1)], s5s, r5s.at[0])
    all_sent(x5.at[pl.ds(0, Z)], f5s, f5r)
    all_sent(r6, s6s, r6s)
    all_sent(three(h7), s7s, r7s)
    all_sent(p8, d8s, d8r)
    all_sent(r8, s8s, r8s)
    all_sent(three_out, s9s, r9s)


def body(
    residual, mixer_gain, w_query, w_forget, w_input, w_outgate, lower_bound, state, head_gain,
    w_mix_out, ffn_gain, w_gate, w_up, w_down,
):
    vmem = pl.BlockSpec(memory_space=pltpu.VMEM)
    hbm = pl.BlockSpec(memory_space=pltpu.HBM)
    V = pltpu.VMEM
    dma = pltpu.SemaphoreType.DMA
    ring = [V((Z, 16, F), bf16), V((Z, 16, F), bf16), V((Z, 16, F), bf16), V((Z - 1, 16, F), bf16)]
    ring8 = [V((Z, N, 8, ROWS), bf16)] * 3 + [V((Z - 1, N, 8, ROWS), bf16)]
    scratch = [
        V((8, 4 * ROWS), bf16), V((1, F), f32), V((1, 128), f32), V((1, 128), f32), V((1, F), f32),
        V((N, 4, F, 128), bf16), V((N, 128, F), bf16), V((N, FFL, F), bf16), V((N, FFL, F), bf16), V((N, FFL, F), bf16),
        V((N, 2, F), f32), V((LOC, 128, 128), f32),
        V((N, 8, ROWS), bf16), V((2 * Z, N, 8, ROWS), bf16), V((N, ROWS, F), f32),
        V((N, LOC, 512), bf16), V((8, ROWS), f32), V((N - 1, LOC, 512), bf16), V((N - 1, 8, ROWS), f32),
        V((128, 128), f32), V((LOC, 128), f32), V((LOC, 128), f32),
        V((N, LOC, 128), bf16),
        V((2, Z, 16, F), f32), *ring,
        V((16, F), bf16), V((2 * Z, 16, F), bf16), V((N, 2 * Z, 8, ROWS), f32),
        V((N, LOC, 2 * FFP), bf16), V((N - 1, LOC, 2 * FFP), bf16), V((N, LOC, FFP), bf16),
        V((2, Z, N, 8, ROWS), f32), *ring8, V((N, 8, ROWS), bf16),
        dma((13,)), dma, *([dma] * 14),
        dma, dma((Z,)), *([dma] * 12),
        dma, dma((Z,)), *([dma] * 12),
    ]
    out, new_state = pl.pallas_call(
        layer_kernel,
        out_shape=(
            jax.ShapeDtypeStruct((8, 4 * ROWS), bf16),
            jax.ShapeDtypeStruct((LOC, 128, 128), f32),
        ),
        in_specs=[hbm] * 14,
        out_specs=(vmem, vmem),
        scratch_shapes=scratch,
        compiler_params=pltpu.CompilerParams(
            collective_id=0, has_side_effects=True, vmem_limit_bytes=24 * 1024 * 1024
        ),
    )(
        *(
            pltpu.with_memory_space_constraint(a, pltpu.HBM)
            for a in (
                residual.T, mixer_gain.reshape(1, F), lower_bound.reshape(1, 128), head_gain.reshape(1, 128),
                ffn_gain.reshape(1, F), w_query, w_forget, w_input, w_outgate, state.reshape(LOC, 128, 128),
                w_mix_out, w_gate.T, w_up.T, w_down,
            )
        ),
    )
    return out.T, new_state.reshape(LOC, 1, 128, 128)


def solution(mesh):
    in_specs = (
        P(None, ("kv", "tp")), P("kv"), P("kv", "tp"), P("kv", "tp"), P("kv", "tp"), P("kv", "tp"), P("tp"),
        P("kv", "tp", None, None), P(), P("tp", "kv"), P("kv"), P("kv", "tp"), P("kv", "tp"), P("tp", "kv"),
    )
    out_specs = (P(None, ("kv", "tp")), P("kv", "tp", None, None))
    return jax.shard_map(body, mesh=mesh, in_specs=in_specs, out_specs=out_specs, check_vma=False)
```

```python
import jax
import jax.numpy as jnp
from jax import lax
from jax.experimental import pallas as pl
from jax.experimental.pallas import tpu as pltpu
from jax.sharding import PartitionSpec as P

D = 4096
EPS = 1e-06
N = 4
Z = 16
ROWS = 128
LOC = 32
F = 256
FFL = 336
FFP = 384
MESH = pl.DeviceIdType.MESH
NT = (((1,), (1,)), ((), ()))
f32 = jnp.float32
bf16 = jnp.bfloat16


def sigmoid(u):
    return 1.0 / (1.0 + jnp.exp(-u))


def silu(u):
    return u * sigmoid(u)


def z_step(j):
    sign = 1 - 2 * lax.rem(j, 2)
    return 8 + sign * ((j + 1) // 2)


def layer_kernel(
    x_hbm, mg_hbm, lb_hbm, hg_hbm, fg_hbm,
    wq_hbm, wf_hbm, wi_hbm, wo_hbm, state_hbm, wm_hbm, wg_hbm, wu_hbm, wd_hbm,
    out_ref, ns,
    x_ref, mg_ref, lb_ref, hg_ref, fg_ref, wp, wm, wg, wu, wd, gains, st,
    xa, x1, xf, s2, sq2, r2, rq2, qfk, vals, ho, n3, t4, s4, r4, own5, x5, xt5,
    s6, r6, h7, t8, p8, d8, s8, r8,
    wsem, stsem, wps, wpr, wms, wmr, wgs, wgr, wus, wur, wds, wdr, gs, gr, s0s, r0s,
    s1s, r1s, f1s, f1r, s2s, r2s, q2s, q2r, s3s, r3s, ms, mr, s4s, r4s,
    s5s, r5s, f5s, f5r, s6s, r6s, s7s, r7s, d8s, d8r, s8s, r8s,
):
    k = lax.axis_index("kv")
    t = lax.axis_index("tp")
    z = t // 2
    c = lax.rem(t, 2)
    o = 1 - c
    y = k // N
    x = lax.rem(k, N)
    mate = 2 * z + o

    def turn(a, r):
        return lax.rem(a + r, N)

    def y_to(r):
        return turn(y, r) * N + x

    def x_to(r):
        return y * N + turn(x, r)

    def z_to(r):
        return lax.rem(z + r, Z)

    def z_from(r):
        return lax.rem(z - r + Z, Z)

    def rcopy(src, dst, ssem, rsem, kk, tt):
        return pltpu.make_async_remote_copy(
            src_ref=src, dst_ref=dst, send_sem=ssem, recv_sem=rsem,
            device_id=(kk, tt), device_id_type=MESH,
        )

    def all_sent(view, ssem, rsem):
        rcopy(view, view, ssem, rsem, k, mate).wait_send()

    def all_here(view, ssem, rsem):
        rcopy(view, view, ssem, rsem, k, mate).wait_recv()

    def three(ref):
        return ref.at[pl.ds(0, N - 1)]

    def greet(kk, tt):
        barrier = pltpu.get_barrier_semaphore()
        pl.semaphore_signal(barrier, inc=1, device_id=(kk, tt), device_id_type=MESH)

    def greet_z(j, _):
        greet(k, 2 * z_to(z_step(j)) + c)
        return 0

    lax.fori_loop(0, Z - 1, greet_z, 0)
    for r in range(1, N):
        greet(y_to(r), t)
        greet(x_to(r), t)
    greet(k, mate)

    loads = [
        pltpu.make_async_copy(src, dst, wsem.at[i])
        for i, (src, dst) in enumerate(
            (
                (wq_hbm, wp.at[y, 0]), (wf_hbm, wp.at[y, 1]), (wi_hbm, wp.at[y, 2]), (wo_hbm, wp.at[y, 3]),
                (wm_hbm, wm.at[c, y]), (wg_hbm, wg.at[y]), (wu_hbm, wu.at[y]), (wd_hbm, wd.at[y]),
                (x_hbm, x_ref), (mg_hbm, mg_ref), (lb_hbm, lb_ref), (hg_hbm, hg_ref), (fg_hbm, fg_ref),
            )
        )
    ]
    for load in loads:
        load.start()
    state_in = pltpu.make_async_copy(state_hbm, st, stsem)
    state_in.start()
    for load in loads:
        load.wait()
    gains[y, 0:1, :] = mg_ref[...]
    gains[y, 1:2, :] = fg_ref[...]
    pl.semaphore_wait(pltpu.get_barrier_semaphore(), (Z - 1) + 2 * (N - 1) + 1)

    for r in range(1, N):
        there = turn(y, r)
        lanes = pl.ds(pl.multiple_of(there * ROWS, ROWS), ROWS)
        rcopy(x_ref.at[:, lanes], xa.at[y], s0s, r0s, y_to(r), t).start()
        rcopy(gains.at[y], gains.at[y], gs, gr, y_to(r), t).start()
    for ref, ss, rs in ((wp, wps, wpr), (wm.at[c], wms, wmr), (wg, wgs, wgr), (wu, wus, wur), (wd, wds, wdr)):
        for r in range(1, N):
            rcopy(ref.at[y], ref.at[y], ss, rs, y_to(r), t).start()
    mine = pl.ds(pl.multiple_of(y * ROWS, ROWS), ROWS)
    xa[y] = x_ref[:, mine]
    all_here(three(xa), s0s, r0s)

    def gather_tp(own, slots, slot, ss, rs, fs, fr):
        def send(j, _):
            r = z_step(j)
            rcopy(own, slots.at[slot(z, c)], ss, rs.at[r], k, 2 * z_to(r) + c).start()
            return 0

        lax.fori_loop(0, Z - 1, send, 0)
        rcopy(own, slots.at[slot(z, c)], fs, fr, k, mate).start()

        def forward(i, _):
            r = z_step(Z - 2 - i)
            src = slot(z_from(r), c)
            rcopy(own, slots.at[src], ss, rs.at[r], k, mate).wait_recv()
            rcopy(slots.at[src], slots.at[src], fs, fr, k, mate).start()
            return 0

        lax.fori_loop(0, Z - 1, forward, 0)
        all_here(slots.at[pl.ds(0, Z)], fs, fr)

    x1[t] = xa[...]
    gather_tp(xa, x1, lambda zz, cc: 2 * zz + cc, s1s, r1s, f1s, f1r)
    all_here(three(gains), gs, gr)
    all_here(three(wp), wps, wpr)

    row = jnp.zeros((1, ROWS), f32)
    scaled = []
    for b in range(N):
        xt = x1[:, b].astype(f32).reshape(F, ROWS)
        row = row + jnp.sum(xt * xt, axis=0, keepdims=True)
        rows = xt.T
        xf[b] = rows
        scaled.append((rows * gains[b, 0:1, :]).astype(bf16))
    sq2[...] = jnp.broadcast_to(row, (8, ROWS))
    for i in range(4):
        part = jnp.dot(scaled[0], wp[0, i], preferred_element_type=f32)
        for b in range(1, N):
            part = part + jnp.dot(scaled[b], wp[b, i], preferred_element_type=f32)
        s2[:, :, 128 * i : 128 * i + 128] = part.astype(bf16).reshape(N, LOC, 128)

    for r in range(1, N):
        rcopy(s2.at[turn(x, r)], r2.at[r - 1], s2s, r2s, x_to(r), t).start()
        rcopy(sq2, rq2.at[r - 1], q2s, q2r, x_to(r), t).start()
    all_here(three(wm.at[c]), wms, wmr)
    rcopy(wm.at[c], wm.at[c], ms, mr, k, mate).start()
    state_in.wait()
    all_here(rq2, q2s, q2r)
    all_here(r2, s2s, r2s)

    sq = sq2[...]
    raw = s2[x].astype(f32)
    for i in range(N - 1):
        sq = sq + rq2[i]
        raw = raw + r2[i].astype(f32)
    lane = lax.broadcasted_iota(jnp.int32, (LOC, ROWS), 1)
    seq = lax.broadcasted_iota(jnp.int32, (LOC, ROWS), 0)
    total = jnp.sum(jnp.where(lane == seq + x * LOC, sq[0:1, :], 0.0), axis=1, keepdims=True)
    raw = raw * lax.rsqrt(total / D + EPS)

    bound = lb_ref[...]
    forget_raw = raw[:, 128:256]
    forget = bound + (1.0 - bound) * sigmoid(forget_raw)
    keyvec = (1.0 - bound) * sigmoid(-forget_raw)
    query = silu(raw[:, 0:128])
    vals[...] = raw[:, 256:384]
    out_gate = silu(raw[:, 384:512])
    qfk[...] = jnp.concatenate([query * forget, forget, keyvec, jnp.zeros((LOC, 128), f32)], axis=0).T
    weight = jnp.sum(query * keyvec, axis=1, keepdims=True)

    for s in range(LOC):
        ho[s : s + 1, :] = jnp.sum(qfk[:, s : s + 1] * st[s], axis=0, keepdims=True)

    head = ho[...] + weight * vals[...]
    inv = lax.rsqrt(jnp.mean(head * head, axis=1, keepdims=True) + EPS)
    n3[2 * x + c] = (head * inv * hg_ref[...] * out_gate).astype(bf16)

    mine3 = n3.at[2 * x + c]
    for r in range(1, N):
        rcopy(mine3, mine3, s3s, r3s, x_to(r), t).start()
        rcopy(mine3, mine3, s3s, r3s, x_to(r), mate).start()
    rcopy(mine3, mine3, s3s, r3s, k, mate).start()
    for s in range(LOC):
        ns[s] = (
            qfk[:, LOC + s : LOC + s + 1] * st[s]
            + qfk[:, 2 * LOC + s : 2 * LOC + s + 1] * vals[s : s + 1, :]
        )
    all_here(wm.at[o], ms, mr)
    all_here(n3.at[pl.ds(0, 2 * N - 1)], s3s, r3s)

    heads = [jnp.concatenate([n3[4 * c + i], n3[4 * c + 2 + i]], axis=0) for i in range(2)]
    for b in range(N):
        mixed = jnp.dot(heads[0], wm[0, b], preferred_element_type=f32)
        mixed = mixed + jnp.dot(heads[1], wm[1, b], preferred_element_type=f32)
        for i in range(4):
            t4[4 * b + i] = mixed[16 * i : 16 * i + 16, :]
            s4[4 * b + i] = mixed[16 * i : 16 * i + 16, :].astype(bf16)

    def block_of(zz, cc):
        return (zz // 4) * 8 + cc * 4 + lax.rem(zz, 4)

    def send4(j, _):
        r = z_step(j)
        zz = z_to(r)
        rcopy(s4.at[zz], r4.at[r - 1], s4s, r4s, k, 2 * zz + c).start()
        return 0

    lax.fori_loop(0, Z - 1, send4, 0)
    block = xf[z // 4, pl.ds(pl.multiple_of(c * 64 + lax.rem(z, 4) * 16, 16), 16), :] + t4[z]
    all_here(r4, s4s, r4s)
    for i in range(Z - 1):
        block = block + r4[i].astype(f32)
    own5[...] = block.astype(bf16)
    x5[block_of(z, c)] = own5[...]
    gather_tp(own5, x5, block_of, s5s, r5s, f5s, f5r)
    all_here(three(wg), wgs, wgr)
    all_here(three(wu), wus, wur)

    squares = jnp.zeros((ROWS, 1), f32)
    scaled = []
    for b in range(N):
        after = x5[8 * b : 8 * b + 8].reshape(ROWS, F).astype(f32)
        squares = squares + jnp.sum(after * after, axis=1, keepdims=True)
        scaled.append((after * gains[b, 1:2, :]).astype(bf16))

    def projected(w):
        acc = lax.dot_general(scaled[0], w[0], NT, preferred_element_type=f32)
        for b in range(1, N):
            acc = acc + lax.dot_general(scaled[b], w[b], NT, preferred_element_type=f32)
        return acc.astype(bf16).reshape(N, LOC, FFL)

    s6[:, :, 0:FFL] = projected(wg)
    s6[:, :, FFP : FFP + FFL] = projected(wu)
    high = squares.astype(bf16).astype(f32)
    spot = lax.broadcasted_iota(jnp.int32, (ROWS, FFP - FFL), 1)
    tail = jnp.where(spot == 0, high, jnp.where(spot == 1, squares - high, 0.0))
    s6[:, :, FFL:FFP] = tail.astype(bf16).reshape(N, LOC, FFP - FFL)
    s6[:, :, FFP + FFL : 2 * FFP] = jnp.zeros((N, LOC, FFP - FFL), bf16)

    for r in range(1, N):
        rcopy(s6.at[turn(x, r)], r6.at[r - 1], s6s, r6s, x_to(r), t).start()
    for b in range(N):
        xt5[b] = x5[8 * b : 8 * b + 8].reshape(ROWS, F).astype(f32).T.reshape(2 * Z, 8, ROWS)
    all_here(r6, s6s, r6s)
    both = s6[x].astype(f32)
    for i in range(N - 1):
        both = both + r6[i].astype(f32)
    total = both[:, FFL : FFL + 1] + both[:, FFL + 1 : FFL + 2]
    inverse = lax.rsqrt(total / D + EPS)
    hidden = silu(both[:, 0:FFP] * inverse) * (both[:, FFP : 2 * FFP] * inverse)
    spot = lax.broadcasted_iota(jnp.int32, (LOC, FFP), 1)
    h7[x] = jnp.where(spot < FFL, hidden, 0.0).astype(bf16)

    for r in range(1, N):
        rcopy(h7.at[x], h7.at[x], s7s, r7s, x_to(r), t).start()
    all_here(three(wd), wds, wdr)
    all_here(three(h7), s7s, r7s)
    hall = h7[...].reshape(ROWS, FFP)[:, 0:FFL]
    for b in range(N):
        down = jnp.dot(hall, wd[b], preferred_element_type=f32).T
        for i in range(2 * Z):
            t8[i % 2, i // 2, b] = down[8 * i : 8 * i + 8, :]

    p8[...] = t8[o].astype(bf16)
    swap = rcopy(p8, d8, d8s, d8r, k, mate)
    swap.start()
    t8[c, z] = t8[c, z] + xt5[:, t]
    swap.wait_recv()
    s8[...] = (t8[c] + d8[...].astype(f32)).astype(bf16)

    def piece(r, q):
        zz = z_to(r)
        there = turn(y, q)
        rcopy(s8.at[zz, there], r8.at[y * Z + r], s8s, r8s, there * N + x, 2 * zz + c).start()

    def send8(j, _):
        for q in range(N):
            piece(z_step(j), q)
        return 0

    lax.fori_loop(0, Z - 1, send8, 0)
    for q in range(1, N):
        piece(0, q)
    r8[y * Z] = s8[z, y]
    pieces = r8.at[pl.ds(0, N * Z - 1)]
    all_here(pieces, s8s, r8s)
    for b in range(N):
        acc = r8[b * Z].astype(f32)
        for i in range(1, Z):
            acc = acc + r8[b * Z + i].astype(f32)
        out_ref[:, ROWS * b : ROWS * b + ROWS] = acc.astype(bf16)

    all_sent(three(xa), s0s, r0s)
    all_sent(three(gains), gs, gr)
    for ref, ss, rs in ((wp, wps, wpr), (wm.at[c], wms, wmr), (wg, wgs, wgr), (wu, wus, wur), (wd, wds, wdr)):
        all_sent(three(ref), ss, rs)
    all_sent(wm.at[c], ms, mr)
    all_sent(x1.at[pl.ds(0, Z - 1)], s1s, r1s.at[0])
    all_sent(x1.at[pl.ds(0, Z)], f1s, f1r)
    all_sent(r2, s2s, r2s)
    all_sent(rq2, q2s, q2r)
    all_sent(n3.at[pl.ds(0, 2 * N - 1)], s3s, r3s)
    all_sent(r4, s4s, r4s)
    all_sent(x5.at[pl.ds(0, Z - 1)], s5s, r5s.at[0])
    all_sent(x5.at[pl.ds(0, Z)], f5s, f5r)
    all_sent(r6, s6s, r6s)
    all_sent(three(h7), s7s, r7s)
    all_sent(p8, d8s, d8r)
    all_sent(pieces, s8s, r8s)


def write_out(out_ref, ns_ref, out_hbm, ns_hbm, sems):
    part = LOC // 4
    copies = [
        pltpu.make_async_copy(ns_ref.at[pl.ds(part * i, part)], ns_hbm.at[pl.ds(part * i, part)], sems.at[i])
        for i in range(4)
    ]
    copies.append(pltpu.make_async_copy(out_ref, out_hbm, sems.at[4]))
    for copy in copies:
        copy.start()
    for copy in copies:
        copy.wait()


def body(
    residual, mixer_gain, w_query, w_forget, w_input, w_outgate, lower_bound, state, head_gain,
    w_mix_out, ffn_gain, w_gate, w_up, w_down,
):
    vmem = pl.BlockSpec(memory_space=pltpu.VMEM)
    hbm = pl.BlockSpec(memory_space=pltpu.HBM)
    V = pltpu.VMEM
    dma = pltpu.SemaphoreType.DMA
    ring8 = [V((Z, N, 8, ROWS), bf16)] * 3 + [V((N * Z, 8, ROWS), bf16)]
    scratch = [
        V((8, 4 * ROWS), bf16), V((1, F), f32), V((1, 128), f32), V((1, 128), f32), V((1, F), f32),
        V((N, 4, F, 128), bf16), V((2, N, 128, F), bf16), V((N, FFL, F), bf16), V((N, FFL, F), bf16), V((N, FFL, F), bf16),
        V((N, 2, F), f32), V((LOC, 128, 128), f32),
        V((N, 8, ROWS), bf16), V((2 * Z, N, 8, ROWS), bf16), V((N, ROWS, F), f32),
        V((N, LOC, 512), bf16), V((8, ROWS), f32), V((N - 1, LOC, 512), bf16), V((N - 1, 8, ROWS), f32),
        V((128, 128), f32), V((LOC, 128), f32), V((LOC, 128), f32),
        V((2 * N, LOC, 128), bf16),
        V((Z, 16, F), f32), V((Z, 16, F), bf16), V((Z - 1, 16, F), bf16),
        V((16, F), bf16), V((2 * Z, 16, F), bf16), V((N, 2 * Z, 8, ROWS), f32),
        V((N, LOC, 2 * FFP), bf16), V((N - 1, LOC, 2 * FFP), bf16), V((N, LOC, FFP), bf16),
        V((2, Z, N, 8, ROWS), f32), *ring8,
        dma((13,)), dma, *([dma] * 14),
        dma, dma((Z,)), *([dma] * 12),
        dma, dma((Z,)), *([dma] * 10),
    ]
    out, new_state = pl.pallas_call(
        layer_kernel,
        out_shape=(
            jax.ShapeDtypeStruct((8, 4 * ROWS), bf16),
            jax.ShapeDtypeStruct((LOC, 128, 128), f32),
        ),
        in_specs=[hbm] * 14,
        out_specs=(vmem, vmem),
        scratch_shapes=scratch,
        compiler_params=pltpu.CompilerParams(
            collective_id=0, has_side_effects=True, vmem_limit_bytes=24 * 1024 * 1024
        ),
    )(
        *(
            pltpu.with_memory_space_constraint(a, pltpu.HBM)
            for a in (
                residual.T, mixer_gain.reshape(1, F), lower_bound.reshape(1, 128), head_gain.reshape(1, 128),
                ffn_gain.reshape(1, F), w_query, w_forget, w_input, w_outgate, state.reshape(LOC, 128, 128),
                w_mix_out, w_gate.T, w_up.T, w_down,
            )
        ),
    )
    out, new_state = pl.pallas_call(
        write_out,
        out_shape=(
            jax.ShapeDtypeStruct((8, 4 * ROWS), bf16),
            jax.ShapeDtypeStruct((LOC, 128, 128), f32),
        ),
        in_specs=[vmem] * 2,
        out_specs=(hbm, hbm),
        scratch_shapes=[dma((5,))],
        compiler_params=pltpu.CompilerParams(vmem_limit_bytes=8 * 1024 * 1024),
    )(out, new_state)
    return out.T, new_state.reshape(LOC, 1, 128, 128)


def solution(mesh):
    in_specs = (
        P(None, ("kv", "tp")), P("kv"), P("kv", "tp"), P("kv", "tp"), P("kv", "tp"), P("kv", "tp"), P("tp"),
        P("kv", "tp", None, None), P(), P("tp", "kv"), P("kv"), P("kv", "tp"), P("kv", "tp"), P("tp", "kv"),
    )
    out_specs = (P(None, ("kv", "tp")), P("kv", "tp", None, None))
    return jax.shard_map(body, mesh=mesh, in_specs=in_specs, out_specs=out_specs, check_vma=False)
```

```python
import jax
import jax.numpy as jnp
from jax import lax
from jax.experimental import pallas as pl
from jax.experimental.pallas import tpu as pltpu
from jax.sharding import PartitionSpec as P

D = 4096
EPS = 1e-06
N = 4
Z = 16
ROWS = 128
LOC = 32
F = 256
FFL = 336
FFP = 384
MESH = pl.DeviceIdType.MESH
NT = (((1,), (1,)), ((), ()))
f32 = jnp.float32
bf16 = jnp.bfloat16


def sigmoid(u):
    return 1.0 / (1.0 + jnp.exp(-u))


def silu(u):
    return u * sigmoid(u)


def z_step(j):
    sign = 1 - 2 * lax.rem(j, 2)
    return 8 + sign * ((j + 1) // 2)


def layer_kernel(
    x_hbm, mg_hbm, lb_hbm, hg_hbm, fg_hbm,
    wq_hbm, wf_hbm, wi_hbm, wo_hbm, state_hbm, wm_hbm, wg_hbm, wu_hbm, wd_hbm,
    out_ref, ns,
    x_ref, mg_ref, lb_ref, hg_ref, fg_ref, wp, wo, wm, wg, wu, wd, gains, st,
    xa, x1, xf, s2, sq2, r2, rq2, s2b, r2b, qfk, vals, ho, n3, t4, s4, r4, own5, x5, xt5,
    s6, r6, h7, t8, p8, d8, s8, r8,
    word, wsem, stsem, wps, wpr, wos, wor, wms, wmr, wgs, wgr, wus, wur, wds, wdr, gs, gr, s0s, r0s, b2s, b2r,
    s1s, r1s, f1s, f1r, s2s, r2s, q2s, q2r, s3s, r3s, ms, mr, s4s, r4s,
    s5s, r5s, f5s, f5r, s6s, r6s, s7s, r7s, d8s, d8r, s8s, r8s,
):
    k = lax.axis_index("kv")
    t = lax.axis_index("tp")
    z = t // 2
    c = lax.rem(t, 2)
    o = 1 - c
    y = k // N
    x = lax.rem(k, N)
    mate = 2 * z + o

    def turn(a, r):
        return lax.rem(a + r, N)

    def y_to(r):
        return turn(y, r) * N + x

    def x_to(r):
        return y * N + turn(x, r)

    def z_to(r):
        return lax.rem(z + r, Z)

    def z_from(r):
        return lax.rem(z - r + Z, Z)

    def rcopy(src, dst, ssem, rsem, kk, tt):
        return pltpu.make_async_remote_copy(
            src_ref=src, dst_ref=dst, send_sem=ssem, recv_sem=rsem,
            device_id=(kk, tt), device_id_type=MESH,
        )

    def all_sent(view, ssem, rsem):
        rcopy(view, view, ssem, rsem, k, mate).wait_send()

    def all_here(view, ssem, rsem):
        rcopy(view, view, ssem, rsem, k, mate).wait_recv()

    def three(ref):
        return ref.at[pl.ds(0, N - 1)]

    def greet(kk, tt):
        barrier = pltpu.get_barrier_semaphore()
        pl.semaphore_signal(barrier, inc=1, device_id=(kk, tt), device_id_type=MESH)

    for d in range(4, 0, -1):
        greet(k, 2 * z_to(d) + c)
        greet(k, 2 * z_to(Z - d) + c)
    for r in range(1, N):
        greet(y_to(r), t)
        greet(x_to(r), t)
    greet(k, mate)

    loads = [
        pltpu.make_async_copy(src, dst, wsem.at[i])
        for i, (src, dst) in enumerate(
            (
                (wq_hbm, wp.at[y, 0]), (wf_hbm, wp.at[y, 1]), (wi_hbm, wp.at[y, 2]), (wo_hbm, wo.at[y]),
                (wm_hbm, wm.at[c, y]), (wg_hbm, wg.at[y]), (wu_hbm, wu.at[y]), (wd_hbm, wd.at[y]),
                (x_hbm, x_ref), (mg_hbm, mg_ref), (lb_hbm, lb_ref), (hg_hbm, hg_ref), (fg_hbm, fg_ref),
            )
        )
    ]
    for load in loads:
        load.start()
    state_in = pltpu.make_async_copy(state_hbm, st, stsem)
    state_in.start()
    for load in loads:
        load.wait()
    gains[y, 0:1, :] = mg_ref[...]
    gains[y, 1:2, :] = fg_ref[...]
    pl.semaphore_wait(pltpu.get_barrier_semaphore(), 8 + 2 * (N - 1) + 1)

    pl.semaphore_signal(word, inc=1, device_id=(k, 2 * z_to(4) + c), device_id_type=MESH)
    pl.semaphore_signal(word, inc=1, device_id=(k, 2 * z_to(Z - 4) + c), device_id_type=MESH)

    for r in range(1, N):
        there = turn(y, r)
        lanes = pl.ds(pl.multiple_of(there * ROWS, ROWS), ROWS)
        rcopy(x_ref.at[:, lanes], xa.at[y], s0s, r0s, y_to(r), t).start()
        rcopy(gains.at[y], gains.at[y], gs, gr, y_to(r), t).start()
    for ref, ss, rs in ((wp, wps, wpr), (wo, wos, wor), (wm.at[c], wms, wmr), (wg, wgs, wgr), (wu, wus, wur), (wd, wds, wdr)):
        for r in range(1, N):
            rcopy(ref.at[y], ref.at[y], ss, rs, y_to(r), t).start()
    mine = pl.ds(pl.multiple_of(y * ROWS, ROWS), ROWS)
    xa[y] = x_ref[:, mine]
    all_here(three(xa), s0s, r0s)
    pl.semaphore_wait(word, 2)

    def gather_tp(own, slots, slot, ss, rs, fs, fr):
        def send(j, _):
            r = z_step(j)
            rcopy(own, slots.at[slot(z, c)], ss, rs.at[r], k, 2 * z_to(r) + c).start()
            return 0

        lax.fori_loop(0, Z - 1, send, 0)
        rcopy(own, slots.at[slot(z, c)], fs, fr, k, mate).start()

        def forward(i, _):
            r = z_step(Z - 2 - i)
            src = slot(z_from(r), c)
            rcopy(own, slots.at[src], ss, rs.at[r], k, mate).wait_recv()
            rcopy(slots.at[src], slots.at[src], fs, fr, k, mate).start()
            return 0

        lax.fori_loop(0, Z - 1, forward, 0)
        all_here(slots.at[pl.ds(0, Z)], fs, fr)

    x1[t] = xa[...]
    gather_tp(xa, x1, lambda zz, cc: 2 * zz + cc, s1s, r1s, f1s, f1r)
    all_here(three(gains), gs, gr)
    all_here(three(wp), wps, wpr)

    row = jnp.zeros((1, ROWS), f32)
    scaled = []
    for b in range(N):
        xt = x1[:, b].astype(f32).reshape(F, ROWS)
        row = row + jnp.sum(xt * xt, axis=0, keepdims=True)
        rows = xt.T
        xf[b] = rows
        scaled.append((rows * gains[b, 0:1, :]).astype(bf16))
    sq2[...] = jnp.broadcast_to(row, (8, ROWS))

    def projection(w):
        part = jnp.dot(scaled[0], w(0), preferred_element_type=f32)
        for b in range(1, N):
            part = part + jnp.dot(scaled[b], w(b), preferred_element_type=f32)
        return part.astype(bf16).reshape(N, LOC, 128)

    for i in range(3):
        s2[:, :, 128 * i : 128 * i + 128] = projection(lambda b, i=i: wp[b, i])

    for r in range(1, N):
        rcopy(s2.at[turn(x, r)], r2.at[r - 1], s2s, r2s, x_to(r), t).start()
        rcopy(sq2, rq2.at[r - 1], q2s, q2r, x_to(r), t).start()
    all_here(three(wo), wos, wor)
    s2b[...] = projection(lambda b: wo[b])
    for r in range(1, N):
        rcopy(s2b.at[turn(x, r)], r2b.at[r - 1], b2s, b2r, x_to(r), t).start()
    all_here(three(wm.at[c]), wms, wmr)
    rcopy(wm.at[c], wm.at[c], ms, mr, k, mate).start()
    state_in.wait()
    all_here(rq2, q2s, q2r)
    all_here(r2, s2s, r2s)

    sq = sq2[...]
    raw = s2[x].astype(f32)
    for i in range(N - 1):
        sq = sq + rq2[i]
        raw = raw + r2[i].astype(f32)
    lane = lax.broadcasted_iota(jnp.int32, (LOC, ROWS), 1)
    seq = lax.broadcasted_iota(jnp.int32, (LOC, ROWS), 0)
    total = jnp.sum(jnp.where(lane == seq + x * LOC, sq[0:1, :], 0.0), axis=1, keepdims=True)
    inv_a = lax.rsqrt(total / D + EPS)
    raw = raw * inv_a

    bound = lb_ref[...]
    forget_raw = raw[:, 128:256]
    forget = bound + (1.0 - bound) * sigmoid(forget_raw)
    keyvec = (1.0 - bound) * sigmoid(-forget_raw)
    query = silu(raw[:, 0:128])
    vals[...] = raw[:, 256:384]
    qfk[...] = jnp.concatenate([query * forget, forget, keyvec, jnp.zeros((LOC, 128), f32)], axis=0).T
    weight = jnp.sum(query * keyvec, axis=1, keepdims=True)

    for s in range(LOC):
        ho[s : s + 1, :] = jnp.sum(qfk[:, s : s + 1] * st[s], axis=0, keepdims=True)

    all_here(r2b, b2s, b2r)
    raw = s2b[x].astype(f32)
    for i in range(N - 1):
        raw = raw + r2b[i].astype(f32)
    out_gate = silu(raw * inv_a)
    head = ho[...] + weight * vals[...]
    inv = lax.rsqrt(jnp.mean(head * head, axis=1, keepdims=True) + EPS)
    n3[2 * x + c] = (head * inv * hg_ref[...] * out_gate).astype(bf16)

    mine3 = n3.at[2 * x + c]
    for r in range(1, N):
        rcopy(mine3, mine3, s3s, r3s, x_to(r), t).start()
        rcopy(mine3, mine3, s3s, r3s, x_to(r), mate).start()
    rcopy(mine3, mine3, s3s, r3s, k, mate).start()
    for s in range(LOC):
        ns[s] = (
            qfk[:, LOC + s : LOC + s + 1] * st[s]
            + qfk[:, 2 * LOC + s : 2 * LOC + s + 1] * vals[s : s + 1, :]
        )
    all_here(wm.at[o], ms, mr)
    all_here(n3.at[pl.ds(0, 2 * N - 1)], s3s, r3s)

    heads = [jnp.concatenate([n3[4 * c + i], n3[4 * c + 2 + i]], axis=0) for i in range(2)]
    for b in range(N):
        mixed = jnp.dot(heads[0], wm[0, b], preferred_element_type=f32)
        mixed = mixed + jnp.dot(heads[1], wm[1, b], preferred_element_type=f32)
        for i in range(4):
            t4[4 * b + i] = mixed[16 * i : 16 * i + 16, :]
            s4[4 * b + i] = mixed[16 * i : 16 * i + 16, :].astype(bf16)

    def block_of(zz, cc):
        return (zz // 4) * 8 + cc * 4 + lax.rem(zz, 4)

    def send4(j, _):
        r = z_step(j)
        zz = z_to(r)
        rcopy(s4.at[zz], r4.at[r - 1], s4s, r4s, k, 2 * zz + c).start()
        return 0

    lax.fori_loop(0, Z - 1, send4, 0)
    block = xf[z // 4, pl.ds(pl.multiple_of(c * 64 + lax.rem(z, 4) * 16, 16), 16), :] + t4[z]
    all_here(r4, s4s, r4s)
    for i in range(Z - 1):
        block = block + r4[i].astype(f32)
    own5[...] = block.astype(bf16)
    x5[block_of(z, c)] = own5[...]
    gather_tp(own5, x5, block_of, s5s, r5s, f5s, f5r)
    all_here(three(wg), wgs, wgr)
    all_here(three(wu), wus, wur)

    squares = jnp.zeros((ROWS, 1), f32)
    scaled = []
    for b in range(N):
        after = x5[8 * b : 8 * b + 8].reshape(ROWS, F).astype(f32)
        squares = squares + jnp.sum(after * after, axis=1, keepdims=True)
        scaled.append((after * gains[b, 1:2, :]).astype(bf16))

    def projected(w):
        acc = lax.dot_general(scaled[0], w[0], NT, preferred_element_type=f32)
        for b in range(1, N):
            acc = acc + lax.dot_general(scaled[b], w[b], NT, preferred_element_type=f32)
        return acc.astype(bf16).reshape(N, LOC, FFL)

    s6[:, 0, :, 0:FFL] = projected(wg)
    s6[:, 1, :, 0:FFL] = projected(wu)
    high = squares.astype(bf16).astype(f32)
    spot = lax.broadcasted_iota(jnp.int32, (ROWS, FFP - FFL), 1)
    tail = jnp.where(spot == 0, high, jnp.where(spot == 1, squares - high, 0.0))
    s6[:, 0, :, FFL:FFP] = tail.astype(bf16).reshape(N, LOC, FFP - FFL)
    s6[:, 1, :, FFL:FFP] = jnp.zeros((N, LOC, FFP - FFL), bf16)

    for r in range(1, N):
        rcopy(s6.at[turn(x, r)], r6.at[r - 1], s6s, r6s, x_to(r), t).start()
    for b in range(N):
        xt5[b] = x5[8 * b : 8 * b + 8].reshape(ROWS, F).astype(f32).T.reshape(2 * Z, 8, ROWS)
    all_here(r6, s6s, r6s)
    gate = s6[x, 0].astype(f32)
    upper = s6[x, 1].astype(f32)
    for i in range(N - 1):
        gate = gate + r6[i, 0].astype(f32)
        upper = upper + r6[i, 1].astype(f32)
    total = gate[:, FFL : FFL + 1] + gate[:, FFL + 1 : FFL + 2]
    inverse = lax.rsqrt(total / D + EPS)
    hidden = silu(gate * inverse) * (upper * inverse)
    spot = lax.broadcasted_iota(jnp.int32, (LOC, FFP), 1)
    h7[x] = jnp.where(spot < FFL, hidden, 0.0).astype(bf16)

    for r in range(1, N):
        rcopy(h7.at[x], h7.at[x], s7s, r7s, x_to(r), t).start()
    all_here(three(wd), wds, wdr)
    all_here(three(h7), s7s, r7s)
    hall = h7[...].reshape(ROWS, FFP)[:, 0:FFL]
    downs = [jnp.dot(hall, wd[b], preferred_element_type=f32).T for b in range(N)]
    swaps = []
    for b in range(N):
        for i in range(Z):
            even, odd = downs[b][16 * i : 16 * i + 8, :], downs[b][16 * i + 8 : 16 * i + 16, :]
            t8[i, b] = jnp.where(c == 0, even, odd)
            p8[b, i] = jnp.where(c == 0, odd, even).astype(bf16)
        swaps.append(rcopy(p8.at[b], d8.at[b], d8s.at[b], d8r.at[b], k, mate))
        swaps[b].start()

    def piece(r, there):
        zz = z_to(r)
        rcopy(s8.at[zz, there], r8.at[y * Z + r], s8s, r8s, there * N + x, 2 * zz + c).start()

    t8[z] = t8[z] + xt5[:, t]
    for b in range(N):
        swaps[b].wait_recv()
        s8[:, b] = (t8[:, b] + d8[b].astype(f32)).astype(bf16)

        def send8(j, _):
            piece(z_step(j), b)
            return 0

        lax.fori_loop(0, Z - 1, send8, 0)
    for q in range(1, N):
        piece(0, turn(y, q))
    r8[y * Z] = s8[z, y]
    pieces = r8.at[pl.ds(0, N * Z - 1)]
    all_here(pieces, s8s, r8s)
    for b in range(N):
        acc = r8[b * Z].astype(f32)
        for i in range(1, Z):
            acc = acc + r8[b * Z + i].astype(f32)
        out_ref[:, ROWS * b : ROWS * b + ROWS] = acc.astype(bf16)

    all_sent(three(xa), s0s, r0s)
    all_sent(three(gains), gs, gr)
    for ref, ss, rs in ((wp, wps, wpr), (wo, wos, wor), (wm.at[c], wms, wmr), (wg, wgs, wgr), (wu, wus, wur), (wd, wds, wdr)):
        all_sent(three(ref), ss, rs)
    all_sent(wm.at[c], ms, mr)
    all_sent(x1.at[pl.ds(0, Z - 1)], s1s, r1s.at[0])
    all_sent(x1.at[pl.ds(0, Z)], f1s, f1r)
    all_sent(r2, s2s, r2s)
    all_sent(r2b, b2s, b2r)
    all_sent(rq2, q2s, q2r)
    all_sent(n3.at[pl.ds(0, 2 * N - 1)], s3s, r3s)
    all_sent(r4, s4s, r4s)
    all_sent(x5.at[pl.ds(0, Z - 1)], s5s, r5s.at[0])
    all_sent(x5.at[pl.ds(0, Z)], f5s, f5r)
    all_sent(r6, s6s, r6s)
    all_sent(three(h7), s7s, r7s)
    for swap in swaps:
        swap.wait_send()
    all_sent(pieces, s8s, r8s)


def write_out(out_ref, ns_ref, out_hbm, ns_hbm, sems):
    part = LOC // 4
    copies = [
        pltpu.make_async_copy(ns_ref.at[pl.ds(part * i, part)], ns_hbm.at[pl.ds(part * i, part)], sems.at[i])
        for i in range(4)
    ]
    copies.append(pltpu.make_async_copy(out_ref, out_hbm, sems.at[4]))
    for copy in copies:
        copy.start()
    for copy in copies:
        copy.wait()


def body(
    residual, mixer_gain, w_query, w_forget, w_input, w_outgate, lower_bound, state, head_gain,
    w_mix_out, ffn_gain, w_gate, w_up, w_down,
):
    vmem = pl.BlockSpec(memory_space=pltpu.VMEM)
    hbm = pl.BlockSpec(memory_space=pltpu.HBM)
    V = pltpu.VMEM
    dma = pltpu.SemaphoreType.DMA
    ring8 = [V((N, Z, 8, ROWS), bf16)] * 2 + [V((Z, N, 8, ROWS), bf16), V((N * Z, 8, ROWS), bf16)]
    scratch = [
        V((8, 4 * ROWS), bf16), V((1, F), f32), V((1, 128), f32), V((1, 128), f32), V((1, F), f32),
        V((N, 3, F, 128), bf16), V((N, F, 128), bf16), V((2, N, 128, F), bf16), V((N, FFL, F), bf16), V((N, FFL, F), bf16), V((N, FFL, F), bf16),
        V((N, 2, F), f32), V((LOC, 128, 128), f32),
        V((N, 8, ROWS), bf16), V((2 * Z, N, 8, ROWS), bf16), V((N, ROWS, F), f32),
        V((N, LOC, 384), bf16), V((8, ROWS), f32), V((N - 1, LOC, 384), bf16), V((N - 1, 8, ROWS), f32),
        V((N, LOC, 128), bf16), V((N - 1, LOC, 128), bf16),
        V((128, 128), f32), V((LOC, 128), f32), V((LOC, 128), f32),
        V((2 * N, LOC, 128), bf16),
        V((Z, 16, F), f32), V((Z, 16, F), bf16), V((Z - 1, 16, F), bf16),
        V((16, F), bf16), V((2 * Z, 16, F), bf16), V((N, 2 * Z, 8, ROWS), f32),
        V((N, 2, LOC, FFP), bf16), V((N - 1, 2, LOC, FFP), bf16), V((N, LOC, FFP), bf16),
        V((Z, N, 8, ROWS), f32), *ring8,
        pltpu.SemaphoreType.REGULAR, dma((13,)), dma, *([dma] * 18),
        dma, dma((Z,)), *([dma] * 12),
        dma, dma((Z,)), *([dma] * 6), dma((N,)), dma((N,)), dma, dma,
    ]
    out, new_state = pl.pallas_call(
        layer_kernel,
        out_shape=(
            jax.ShapeDtypeStruct((8, 4 * ROWS), bf16),
            jax.ShapeDtypeStruct((LOC, 128, 128), f32),
        ),
        in_specs=[hbm] * 14,
        out_specs=(vmem, vmem),
        scratch_shapes=scratch,
        compiler_params=pltpu.CompilerParams(
            collective_id=0, has_side_effects=True, vmem_limit_bytes=24 * 1024 * 1024
        ),
    )(
        *(
            pltpu.with_memory_space_constraint(a, pltpu.HBM)
            for a in (
                residual.T, mixer_gain.reshape(1, F), lower_bound.reshape(1, 128), head_gain.reshape(1, 128),
                ffn_gain.reshape(1, F), w_query, w_forget, w_input, w_outgate, state.reshape(LOC, 128, 128),
                w_mix_out, w_gate.T, w_up.T, w_down,
            )
        ),
    )
    out, new_state = pl.pallas_call(
        write_out,
        out_shape=(
            jax.ShapeDtypeStruct((8, 4 * ROWS), bf16),
            jax.ShapeDtypeStruct((LOC, 128, 128), f32),
        ),
        in_specs=[vmem] * 2,
        out_specs=(hbm, hbm),
        scratch_shapes=[dma((5,))],
        compiler_params=pltpu.CompilerParams(vmem_limit_bytes=8 * 1024 * 1024),
    )(out, new_state)
    return out.T, new_state.reshape(LOC, 1, 128, 128)


def solution(mesh):
    in_specs = (
        P(None, ("kv", "tp")), P("kv"), P("kv", "tp"), P("kv", "tp"), P("kv", "tp"), P("kv", "tp"), P("tp"),
        P("kv", "tp", None, None), P(), P("tp", "kv"), P("kv"), P("kv", "tp"), P("kv", "tp"), P("tp", "kv"),
    )
    out_specs = (P(None, ("kv", "tp")), P("kv", "tp", None, None))
    return jax.shard_map(body, mesh=mesh, in_specs=in_specs, out_specs=out_specs, check_vma=False)
```

```python
import jax
import jax.numpy as jnp
from jax import lax
from jax.experimental import pallas as pl
from jax.experimental.pallas import tpu as pltpu
from jax.sharding import PartitionSpec as P

D = 4096
EPS = 1e-06
N = 4
Z = 16
ROWS = 128
LOC = 32
F = 256
FFL = 336
FFP = 384
MESH = pl.DeviceIdType.MESH
NT = (((1,), (1,)), ((), ()))
f32 = jnp.float32
bf16 = jnp.bfloat16


def sigmoid(u):
    return 1.0 / (1.0 + jnp.exp(-u))


def silu(u):
    return u * sigmoid(u)


def layer_kernel(
    x_hbm, mg_hbm, lb_hbm, hg_hbm, fg_hbm,
    wq_hbm, wf_hbm, wi_hbm, wo_hbm, state_hbm, wm_hbm, wg_hbm, wu_hbm, wd_hbm,
    out_ref, ns,
    x_ref, mg_ref, lb_ref, hg_ref, fg_ref, wp, wo, wm, wgu, wd, gains, st,
    xa, x1, xf, s2, sq2, r2, rq2, s2b, r2b, qfk, vals, ho, n3, t4, s4, r4, own5, x5, xt5,
    s6, r6, h7, t8, p8, d8, s8, r8,
    word, wsem, psem, gsem, stsem, wps, wpr, wos, wor, wms, wmr, wgs, wgr, wds, wdr, gr, r0, ms, mr,
    out_a, out_b, out_c, ring, fwd, in_a, in_b, in_c, r4s, d8s, d8r, r8s,
):
    k = lax.axis_index("kv")
    t = lax.axis_index("tp")
    z = t // 2
    c = lax.rem(t, 2)
    o = 1 - c
    y = k // N
    x = lax.rem(k, N)
    mate = 2 * z + o

    def turn(a, r):
        return lax.rem(a + r, N)

    def y_to(r):
        return turn(y, r) * N + x

    def x_to(r):
        return y * N + turn(x, r)

    def z_to(r):
        return lax.rem(z + r, Z)

    def z_from(r):
        return lax.rem(z - r + Z, Z)

    def rcopy(src, dst, ssem, rsem, kk, tt):
        return pltpu.make_async_remote_copy(
            src_ref=src, dst_ref=dst, send_sem=ssem, recv_sem=rsem,
            device_id=(kk, tt), device_id_type=MESH,
        )

    def all_sent(view, ssem, rsem):
        rcopy(view, view, ssem, rsem, k, mate).wait_send()

    def all_here(view, ssem, rsem):
        rcopy(view, view, ssem, rsem, k, mate).wait_recv()

    def unit(n):
        return r8.at[pl.ds(0, n)]

    def three(ref):
        return ref.at[pl.ds(0, N - 1)]

    def greet(kk, tt):
        barrier = pltpu.get_barrier_semaphore()
        pl.semaphore_signal(barrier, inc=1, device_id=(kk, tt), device_id_type=MESH)

    for d in range(4, 0, -1):
        greet(k, 2 * z_to(d) + c)
        greet(k, 2 * z_to(Z - d) + c)
    for r in range(1, N):
        greet(y_to(r), t)
        greet(x_to(r), t)
    greet(k, mate)

    places = {
        "x": (x_hbm, x_ref), "mg": (mg_hbm, mg_ref), "fg": (fg_hbm, fg_ref),
        "o": (wo_hbm, wo.at[y]),
        "m": (wm_hbm, wm.at[c, y]), "d": (wd_hbm, wd.at[y]),
        "lb": (lb_hbm, lb_ref), "hg": (hg_hbm, hg_ref),
    }

    def pass_on(sem, d):
        for r in (d, Z - d):
            pl.semaphore_signal(sem, inc=1, device_id=(k, 2 * z_to(r) + c), device_id_type=MESH)

    loads = {
        name: pltpu.make_async_copy(src, dst, wsem.at[i]) for i, (name, (src, dst)) in enumerate(places.items())
    }
    for i, src in enumerate((wq_hbm, wf_hbm, wi_hbm)):
        pltpu.make_async_copy(src, wp.at[y, i], psem).start()
    for load in loads.values():
        load.start()
    for i, src in enumerate((wg_hbm, wu_hbm)):
        pltpu.make_async_copy(src, wgu.at[y, i], gsem).start()
    loads["p"] = pltpu.make_async_copy(wp.at[y], wp.at[y], psem)
    loads["g"] = pltpu.make_async_copy(wgu.at[y], wgu.at[y], gsem)
    loads["x"].wait()
    pl.semaphore_wait(pltpu.get_barrier_semaphore(), 8 + 2 * (N - 1) + 1)
    for r in range(1, N):
        there = turn(y, r)
        lanes = pl.ds(pl.multiple_of(there * ROWS, ROWS), ROWS)
        rcopy(x_ref.at[:, lanes], xa.at[y], out_a, r0, y_to(r), t).start()
    pass_on(word, 4)
    loads["mg"].wait()
    loads["fg"].wait()
    gains[y, 0:1, :] = mg_ref[...]
    gains[y, 1:2, :] = fg_ref[...]
    for r in range(1, N):
        rcopy(gains.at[y], gains.at[y], out_a, gr, y_to(r), t).start()
    weights = (
        ("p", wp, wps, wpr), ("o", wo, wos, wor), ("m", wm.at[c], wms, wmr), ("g", wgu, wgs, wgr), ("d", wd, wds, wdr),
    )

    def send_weights(name, ref, ss, rs):
        third = FFL // 3
        if name == "p":
            parts = [ref.at[y, i] for i in range(3)]
        elif name == "g":
            parts = [ref.at[y, i, pl.ds(third * j, third)] for i in range(2) for j in range(3)]
        elif name == "d":
            parts = [ref.at[y, pl.ds(third * j, third)] for j in range(3)]
        else:
            parts = [ref.at[y]]
        for part in parts:
            for r in range(1, N):
                rcopy(part, part, ss, rs, y_to(r), t).start()

    for name, ref, ss, rs in weights:
        loads[name].wait()
        send_weights(name, ref, ss, rs)
    state_in = pltpu.make_async_copy(state_hbm, st, stsem)
    state_in.start()
    loads["lb"].wait()
    loads["hg"].wait()
    mine = pl.ds(pl.multiple_of(y * ROWS, ROWS), ROWS)
    xa[y] = x_ref[:, mine]
    all_here(three(xa), out_a, r0)

    def ways(d):
        return (d, Z - d) if d < 8 else (8,)

    def to_far(own, slots, slot, out):
        for d in range(8, 0, -1):
            for r in ways(d):
                rcopy(own, slots.at[slot(z, c)], out, ring.at[d - 1], k, 2 * z_to(r) + c).start()

    def pass_to_mate(own, slots, slot, out):
        rcopy(own, slots.at[slot(z, c)], out, fwd, k, mate).start()
        for d in range(1, 9):
            all_here(slots.at[pl.ds(0, len(ways(d)))], out, ring.at[d - 1])
            for r in ways(d):
                src = slots.at[slot(z_from(r), c)]
                rcopy(src, src, out, fwd, k, mate).start()
        all_here(slots.at[pl.ds(0, Z)], out, fwd)

    x1[t] = xa[...]

    def by_tp(zz, cc):
        return 2 * zz + cc

    pl.semaphore_wait(word, 2)
    to_far(xa, x1, by_tp, out_b)
    pass_to_mate(xa, x1, by_tp, out_b)
    all_here(three(gains), out_a, gr)
    all_here(three(wp), wps, wpr)

    row = jnp.zeros((1, ROWS), f32)
    scaled = []
    for b in range(N):
        xt = x1[:, b].astype(f32).reshape(F, ROWS)
        row = row + jnp.sum(xt * xt, axis=0, keepdims=True)
        rows = xt.T
        xf[b] = rows
        scaled.append((rows * gains[b, 0:1, :]).astype(bf16))
    sq2[...] = jnp.broadcast_to(row, (8, ROWS))

    def projection(w):
        part = jnp.dot(scaled[0], w(0), preferred_element_type=f32)
        for b in range(1, N):
            part = part + jnp.dot(scaled[b], w(b), preferred_element_type=f32)
        return part.astype(bf16).reshape(N, LOC, 128)

    for i in range(3):
        s2[:, :, 128 * i : 128 * i + 128] = projection(lambda b, i=i: wp[b, i])

    for r in range(1, N):
        rcopy(s2.at[turn(x, r)], r2.at[r - 1], out_c, in_a, x_to(r), t).start()
        rcopy(sq2, rq2.at[r - 1], out_c, in_a, x_to(r), t).start()
    all_here(three(wo), wos, wor)
    s2b[...] = projection(lambda b: wo[b])
    for r in range(1, N):
        rcopy(s2b.at[turn(x, r)], r2b.at[r - 1], out_c, in_b, x_to(r), t).start()
    state_in.wait()
    all_here(unit(42), out_c, in_a)

    sq = sq2[...]
    raw = s2[x].astype(f32)
    for i in range(N - 1):
        sq = sq + rq2[i]
        raw = raw + r2[i].astype(f32)
    lane = lax.broadcasted_iota(jnp.int32, (LOC, ROWS), 1)
    seq = lax.broadcasted_iota(jnp.int32, (LOC, ROWS), 0)
    total = jnp.sum(jnp.where(lane == seq + x * LOC, sq[0:1, :], 0.0), axis=1, keepdims=True)
    inv_a = lax.rsqrt(total / D + EPS)
    raw = raw * inv_a

    bound = lb_ref[...]
    forget_raw = raw[:, 128:256]
    forget = bound + (1.0 - bound) * sigmoid(forget_raw)
    keyvec = (1.0 - bound) * sigmoid(-forget_raw)
    query = silu(raw[:, 0:128])
    vals[...] = raw[:, 256:384]
    qfk[...] = jnp.concatenate([query * forget, forget, keyvec, jnp.zeros((LOC, 128), f32)], axis=0).T
    weight = jnp.sum(query * keyvec, axis=1, keepdims=True)

    for s in range(LOC):
        ho[s : s + 1, :] = jnp.sum(qfk[:, s : s + 1] * st[s], axis=0, keepdims=True)

    all_here(r2b, out_c, in_b)
    raw = s2b[x].astype(f32)
    for i in range(N - 1):
        raw = raw + r2b[i].astype(f32)
    out_gate = silu(raw * inv_a)
    head = ho[...] + weight * vals[...]
    inv = lax.rsqrt(jnp.mean(head * head, axis=1, keepdims=True) + EPS)
    n3[2 * x + c] = (head * inv * hg_ref[...] * out_gate).astype(bf16)

    mine3 = n3.at[2 * x + c]
    all_sent(unit(6), out_a, in_c)
    for r in range(1, N):
        rcopy(mine3, mine3, out_a, in_c, x_to(r), t).start()
        rcopy(mine3, mine3, out_a, in_c, x_to(r), mate).start()
    rcopy(mine3, mine3, out_a, in_c, k, mate).start()
    all_here(three(wm.at[c]), wms, wmr)
    rcopy(wm.at[c], wm.at[c], ms, mr, k, mate).start()
    for s in range(LOC):
        ns[s] = (
            qfk[:, LOC + s : LOC + s + 1] * st[s]
            + qfk[:, 2 * LOC + s : 2 * LOC + s + 1] * vals[s : s + 1, :]
        )
    all_here(wm.at[o], ms, mr)
    all_here(n3.at[pl.ds(0, 2 * N - 1)], out_a, in_c)

    heads = [jnp.concatenate([n3[4 * c + i], n3[4 * c + 2 + i]], axis=0) for i in range(2)]
    for b in range(N):
        mixed = jnp.dot(heads[0], wm[0, b], preferred_element_type=f32)
        mixed = mixed + jnp.dot(heads[1], wm[1, b], preferred_element_type=f32)
        for i in range(4):
            t4[4 * b + i] = mixed[16 * i : 16 * i + 16, :]
            s4[4 * b + i] = mixed[16 * i : 16 * i + 16, :].astype(bf16)

    def block_of(zz, cc):
        return (zz // 4) * 8 + cc * 4 + lax.rem(zz, 4)

    all_sent(x1.at[pl.ds(0, 2 * Z - 1)], out_b, in_c)
    for d in range(8, 0, -1):
        for r in ways(d):
            rcopy(s4.at[z_to(r)], r4.at[r - 1], out_b, r4s, k, 2 * z_to(r) + c).start()
    block = xf[z // 4, pl.ds(pl.multiple_of(c * 64 + lax.rem(z, 4) * 16, 16), 16), :] + t4[z]
    all_here(r4, out_b, r4s)
    for i in range(Z - 1):
        block = block + r4[i].astype(f32)
    own5[...] = block.astype(bf16)
    x5[block_of(z, c)] = own5[...]
    all_sent(unit(54), out_c, r4s)
    to_far(own5, x5, block_of, out_c)
    pass_to_mate(own5, x5, block_of, out_c)
    all_here(three(wgu), wgs, wgr)

    squares = jnp.zeros((ROWS, 1), f32)
    scaled = []
    for b in range(N):
        after = x5[8 * b : 8 * b + 8].reshape(ROWS, F).astype(f32)
        squares = squares + jnp.sum(after * after, axis=1, keepdims=True)
        scaled.append((after * gains[b, 1:2, :]).astype(bf16))

    def projected(i):
        acc = lax.dot_general(scaled[0], wgu[0, i], NT, preferred_element_type=f32)
        for b in range(1, N):
            acc = acc + lax.dot_general(scaled[b], wgu[b, i], NT, preferred_element_type=f32)
        return acc.astype(bf16).reshape(N, LOC, FFL)

    s6[:, 0, :, 0:FFL] = projected(0)
    s6[:, 1, :, 0:FFL] = projected(1)
    high = squares.astype(bf16).astype(f32)
    spot = lax.broadcasted_iota(jnp.int32, (ROWS, FFP - FFL), 1)
    tail = jnp.where(spot == 0, high, jnp.where(spot == 1, squares - high, 0.0))
    s6[:, 0, :, FFL:FFP] = tail.astype(bf16).reshape(N, LOC, FFP - FFL)
    s6[:, 1, :, FFL:FFP] = jnp.zeros((N, LOC, FFP - FFL), bf16)

    all_sent(unit(28), out_a, in_a)
    for r in range(1, N):
        rcopy(s6.at[turn(x, r)], r6.at[r - 1], out_a, in_a, x_to(r), t).start()
    for b in range(N):
        xt5[b] = x5[8 * b : 8 * b + 8].reshape(ROWS, F).astype(f32).T.reshape(2 * Z, 8, ROWS)
    all_here(r6, out_a, in_a)
    gate = s6[x, 0].astype(f32)
    upper = s6[x, 1].astype(f32)
    for i in range(N - 1):
        gate = gate + r6[i, 0].astype(f32)
        upper = upper + r6[i, 1].astype(f32)
    total = gate[:, FFL : FFL + 1] + gate[:, FFL + 1 : FFL + 2]
    inverse = lax.rsqrt(total / D + EPS)
    hidden = silu(gate * inverse) * (upper * inverse)
    spot = lax.broadcasted_iota(jnp.int32, (LOC, FFP), 1)
    h7[x] = jnp.where(spot < FFL, hidden, 0.0).astype(bf16)

    all_sent(unit(60), out_b, in_b)
    for r in range(1, N):
        rcopy(h7.at[x], h7.at[x], out_b, in_b, x_to(r), t).start()
    all_here(three(wd), wds, wdr)
    all_here(three(h7), out_b, in_b)
    hall = h7[...].reshape(ROWS, FFP)[:, 0:FFL]
    downs = [jnp.dot(hall, wd[b], preferred_element_type=f32).T for b in range(N)]
    swaps = []
    for b in range(N):
        for i in range(Z):
            even, odd = downs[b][16 * i : 16 * i + 8, :], downs[b][16 * i + 8 : 16 * i + 16, :]
            t8[i, b] = jnp.where(c == 0, even, odd)
            p8[b, i] = jnp.where(c == 0, odd, even).astype(bf16)
        swaps.append(rcopy(p8.at[b], d8.at[b], d8s, d8r.at[b], k, mate))
        swaps[b].start()

    all_sent(x5.at[pl.ds(0, 2 * Z - 1)], out_c, in_b)

    def piece(r, there):
        zz = z_to(r)
        rcopy(s8.at[zz, there], r8.at[y * Z + r], out_c, r8s, there * N + x, 2 * zz + c).start()

    t8[z] = t8[z] + xt5[:, t]
    for b in range(N):
        swaps[b].wait_recv()
        s8[:, b] = (t8[:, b] + d8[b].astype(f32)).astype(bf16)
        for d in range(8, 0, -1):
            for r in ways(d):
                piece(r, b)
    for q in range(1, N):
        piece(0, turn(y, q))
    r8[y * Z] = s8[z, y]
    all_here(unit(N * Z - 1), out_c, r8s)
    for b in range(N):
        acc = r8[b * Z].astype(f32)
        for i in range(1, Z):
            acc = acc + r8[b * Z + i].astype(f32)
        out_ref[:, ROWS * b : ROWS * b + ROWS] = acc.astype(bf16)

    for _, ref, ss, rs in weights:
        all_sent(three(ref), ss, rs)
    all_sent(wm.at[c], ms, mr)
    all_sent(unit(N * Z), d8s, r8s)
    all_sent(r6, out_a, in_a)
    all_sent(three(h7), out_b, in_b)
    all_sent(unit(N * Z - 1), out_c, r8s)


def write_out(out_ref, ns_ref, out_hbm, ns_hbm, sems):
    part = LOC // 4
    copies = [
        pltpu.make_async_copy(ns_ref.at[pl.ds(part * i, part)], ns_hbm.at[pl.ds(part * i, part)], sems.at[i])
        for i in range(4)
    ]
    copies.append(pltpu.make_async_copy(out_ref, out_hbm, sems.at[4]))
    for copy in copies:
        copy.start()
    for copy in copies:
        copy.wait()


def body(
    residual, mixer_gain, w_query, w_forget, w_input, w_outgate, lower_bound, state, head_gain,
    w_mix_out, ffn_gain, w_gate, w_up, w_down,
):
    vmem = pl.BlockSpec(memory_space=pltpu.VMEM)
    hbm = pl.BlockSpec(memory_space=pltpu.HBM)
    V = pltpu.VMEM
    dma = pltpu.SemaphoreType.DMA
    ring8 = [V((N, Z, 8, ROWS), bf16)] * 2 + [V((Z, N, 8, ROWS), bf16), V((N * Z, 8, ROWS), bf16)]
    scratch = [
        V((8, 4 * ROWS), bf16), V((1, F), f32), V((1, 128), f32), V((1, 128), f32), V((1, F), f32),
        V((N, 3, F, 128), bf16), V((N, F, 128), bf16), V((2, N, 128, F), bf16), V((N, 2, FFL, F), bf16), V((N, FFL, F), bf16),
        V((N, 2, F), f32), V((LOC, 128, 128), f32),
        V((N, 8, ROWS), bf16), V((2 * Z, N, 8, ROWS), bf16), V((N, ROWS, F), f32),
        V((N, LOC, 384), bf16), V((8, ROWS), f32), V((N - 1, LOC, 384), bf16), V((N - 1, 8, ROWS), f32),
        V((N, LOC, 128), bf16), V((N - 1, LOC, 128), bf16),
        V((128, 128), f32), V((LOC, 128), f32), V((LOC, 128), f32),
        V((2 * N, LOC, 128), bf16),
        V((Z, 16, F), f32), V((Z, 16, F), bf16), V((Z - 1, 16, F), bf16),
        V((16, F), bf16), V((2 * Z, 16, F), bf16), V((N, 2 * Z, 8, ROWS), f32),
        V((N, 2, LOC, FFP), bf16), V((N - 1, 2, LOC, FFP), bf16), V((N, LOC, FFP), bf16),
        V((Z, N, 8, ROWS), f32), *ring8,
        pltpu.SemaphoreType.REGULAR, dma((8,)), *([dma] * 17),
        dma, dma, dma, dma((8,)), *([dma] * 6), dma((N,)), dma,
    ]
    out, new_state = pl.pallas_call(
        layer_kernel,
        out_shape=(
            jax.ShapeDtypeStruct((8, 4 * ROWS), bf16),
            jax.ShapeDtypeStruct((LOC, 128, 128), f32),
        ),
        in_specs=[hbm] * 14,
        out_specs=(vmem, vmem),
        scratch_shapes=scratch,
        compiler_params=pltpu.CompilerParams(
            collective_id=0, has_side_effects=True, vmem_limit_bytes=24 * 1024 * 1024
        ),
    )(
        *(
            pltpu.with_memory_space_constraint(a, pltpu.HBM)
            for a in (
                residual.T, mixer_gain.reshape(1, F), lower_bound.reshape(1, 128), head_gain.reshape(1, 128),
                ffn_gain.reshape(1, F), w_query, w_forget, w_input, w_outgate, state.reshape(LOC, 128, 128),
                w_mix_out, w_gate.T, w_up.T, w_down,
            )
        ),
    )
    out, new_state = pl.pallas_call(
        write_out,
        out_shape=(
            jax.ShapeDtypeStruct((8, 4 * ROWS), bf16),
            jax.ShapeDtypeStruct((LOC, 128, 128), f32),
        ),
        in_specs=[vmem] * 2,
        out_specs=(hbm, hbm),
        scratch_shapes=[dma((5,))],
        compiler_params=pltpu.CompilerParams(vmem_limit_bytes=8 * 1024 * 1024),
    )(out, new_state)
    return out.T, new_state.reshape(LOC, 1, 128, 128)


def solution(mesh):
    in_specs = (
        P(None, ("kv", "tp")), P("kv"), P("kv", "tp"), P("kv", "tp"), P("kv", "tp"), P("kv", "tp"), P("tp"),
        P("kv", "tp", None, None), P(), P("tp", "kv"), P("kv"), P("kv", "tp"), P("kv", "tp"), P("tp", "kv"),
    )
    out_specs = (P(None, ("kv", "tp")), P("kv", "tp", None, None))
    return jax.shard_map(body, mesh=mesh, in_specs=in_specs, out_specs=out_specs, check_vma=False)
```

```python
import jax
import jax.numpy as jnp
from jax import lax
from jax.experimental import pallas as pl
from jax.experimental.pallas import tpu as pltpu
from jax.sharding import PartitionSpec as P

D = 4096
EPS = 1e-06
N = 4
Z = 16
ROWS = 128
LOC = 32
F = 256
FFL = 336
FFP = 384
MESH = pl.DeviceIdType.MESH
NT = (((1,), (1,)), ((), ()))
f32 = jnp.float32
bf16 = jnp.bfloat16


def sigmoid(u):
    return 1.0 / (1.0 + jnp.exp(-u))


def silu(u):
    return u * sigmoid(u)


def layer_kernel(
    x_hbm, mg_hbm, lb_hbm, hg_hbm, fg_hbm,
    wq_hbm, wf_hbm, wi_hbm, wo_hbm, state_hbm, wm_hbm, wg_hbm, wu_hbm, wd_hbm,
    out_ref, ns,
    x_ref, mg_ref, lb_ref, hg_ref, fg_ref, wp, wo, wm, wgu, wd, gains, st,
    xa, x1, xf, s2, sq2, r2, rq2, s2b, r2b, qfk, vals, ho, n3, t4, s4, r4, own5, x5, xt5,
    s6, r6, h7, t8, p8, d8, s8, r8,
    word, wsem, psem, gsem, stsem, wps, wpr, wos, wor, wms, wmr, wgs, wgr, wds, wdr, gr, r0, ms, mr,
    out_a, out_b, out_c, ring, fwd, in_a, in_b, in_c, r4s, d8s, d8r, r8s,
):
    k = lax.axis_index("kv")
    t = lax.axis_index("tp")
    z = t // 2
    c = lax.rem(t, 2)
    o = 1 - c
    y = k // N
    x = lax.rem(k, N)
    mate = 2 * z + o

    def turn(a, r):
        return lax.rem(a + r, N)

    def y_to(r):
        return turn(y, r) * N + x

    def x_to(r):
        return y * N + turn(x, r)

    def z_to(r):
        return lax.rem(z + r, Z)

    def z_from(r):
        return lax.rem(z - r + Z, Z)

    def rcopy(src, dst, ssem, rsem, kk, tt):
        return pltpu.make_async_remote_copy(
            src_ref=src, dst_ref=dst, send_sem=ssem, recv_sem=rsem,
            device_id=(kk, tt), device_id_type=MESH,
        )

    def all_sent(view, ssem, rsem):
        rcopy(view, view, ssem, rsem, k, mate).wait_send()

    def all_here(view, ssem, rsem):
        rcopy(view, view, ssem, rsem, k, mate).wait_recv()

    def unit(n):
        return r8.at[pl.ds(0, n)]

    def three(ref):
        return ref.at[pl.ds(0, N - 1)]

    def greet(kk, tt):
        barrier = pltpu.get_barrier_semaphore()
        pl.semaphore_signal(barrier, inc=1, device_id=(kk, tt), device_id_type=MESH)

    for d in range(4, 0, -1):
        greet(k, 2 * z_to(d) + c)
        greet(k, 2 * z_to(Z - d) + c)
    for r in (2, 1, 3):
        greet(y_to(r), t)
        greet(x_to(r), t)
    greet(k, mate)

    places = {
        "x": (x_hbm, x_ref), "mg": (mg_hbm, mg_ref), "fg": (fg_hbm, fg_ref),
        "o": (wo_hbm, wo.at[y]),
        "m": (wm_hbm, wm.at[c, y]), "d": (wd_hbm, wd.at[y]),
        "lb": (lb_hbm, lb_ref), "hg": (hg_hbm, hg_ref),
    }

    def pass_on(sem, d):
        for r in (d, Z - d):
            pl.semaphore_signal(sem, inc=1, device_id=(k, 2 * z_to(r) + c), device_id_type=MESH)

    loads = {
        name: pltpu.make_async_copy(src, dst, wsem.at[i]) for i, (name, (src, dst)) in enumerate(places.items())
    }
    for i, src in enumerate((wq_hbm, wf_hbm, wi_hbm)):
        pltpu.make_async_copy(src, wp.at[y, i], psem).start()
    for load in loads.values():
        load.start()
    for i, src in enumerate((wg_hbm, wu_hbm)):
        pltpu.make_async_copy(src, wgu.at[y, i], gsem).start()
    loads["p"] = pltpu.make_async_copy(wp.at[y], wp.at[y], psem)
    loads["g"] = pltpu.make_async_copy(wgu.at[y], wgu.at[y], gsem)
    loads["x"].wait()
    pl.semaphore_wait(pltpu.get_barrier_semaphore(), 8 + 2 * (N - 1) + 1)
    for r in (2, 1, 3):
        there = turn(y, r)
        lanes = pl.ds(pl.multiple_of(there * ROWS, ROWS), ROWS)
        rcopy(x_ref.at[:, lanes], xa.at[y], out_a, r0, y_to(r), t).start()
    pass_on(word, 4)
    loads["mg"].wait()
    loads["fg"].wait()
    gains[y, 0:1, :] = mg_ref[...]
    gains[y, 1:2, :] = fg_ref[...]
    for r in (2, 1, 3):
        rcopy(gains.at[y], gains.at[y], out_a, gr, y_to(r), t).start()
    weights = (
        ("p", wp, wps, wpr), ("o", wo, wos, wor), ("m", wm.at[c], wms, wmr), ("g", wgu, wgs, wgr), ("d", wd, wds, wdr),
    )

    def send_weights(name, ref, ss, rs):
        third = FFL // 3
        if name == "p":
            parts = [ref.at[y, i] for i in range(3)]
        elif name == "g":
            parts = [ref.at[y, i, pl.ds(third * j, third)] for i in range(2) for j in range(3)]
        elif name == "d":
            parts = [ref.at[y, pl.ds(third * j, third)] for j in range(3)]
        else:
            parts = [ref.at[y]]
        for part in parts:
            for r in (2, 1, 3):
                rcopy(part, part, ss, rs, y_to(r), t).start()

    for name, ref, ss, rs in weights:
        loads[name].wait()
        send_weights(name, ref, ss, rs)
    state_in = pltpu.make_async_copy(state_hbm, st, stsem)
    state_in.start()
    loads["lb"].wait()
    loads["hg"].wait()
    mine = pl.ds(pl.multiple_of(y * ROWS, ROWS), ROWS)
    xa[y] = x_ref[:, mine]
    all_here(three(xa), out_a, r0)

    def ways(d):
        return (d, Z - d) if d < 8 else (8,)

    def to_far(own, slots, slot, out):
        for d in range(8, 0, -1):
            for r in ways(d):
                rcopy(own, slots.at[slot(z, c)], out, ring.at[d - 1], k, 2 * z_to(r) + c).start()

    def pass_to_mate(own, slots, slot, out):
        rcopy(own, slots.at[slot(z, c)], out, fwd, k, mate).start()
        for d in range(1, 9):
            all_here(slots.at[pl.ds(0, len(ways(d)))], out, ring.at[d - 1])
            for r in ways(d):
                src = slots.at[slot(z_from(r), c)]
                rcopy(src, src, out, fwd, k, mate).start()
        all_here(slots.at[pl.ds(0, Z)], out, fwd)

    x1[t] = xa[...]

    def by_tp(zz, cc):
        return 2 * zz + cc

    pl.semaphore_wait(word, 2)
    to_far(xa, x1, by_tp, out_b)
    pass_to_mate(xa, x1, by_tp, out_b)
    all_here(three(gains), out_a, gr)
    all_here(three(wp), wps, wpr)

    row = jnp.zeros((1, ROWS), f32)
    scaled = []
    for b in range(N):
        xt = x1[:, b].astype(f32).reshape(F, ROWS)
        row = row + jnp.sum(xt * xt, axis=0, keepdims=True)
        rows = xt.T
        xf[b] = rows
        scaled.append((rows * gains[b, 0:1, :]).astype(bf16))
    sq2[...] = jnp.broadcast_to(row, (8, ROWS))

    def projection(w):
        part = jnp.dot(scaled[0], w(0), preferred_element_type=f32)
        for b in range(1, N):
            part = part + jnp.dot(scaled[b], w(b), preferred_element_type=f32)
        return part.astype(bf16).reshape(N, LOC, 128)

    for i in range(3):
        s2[:, :, 128 * i : 128 * i + 128] = projection(lambda b, i=i: wp[b, i])

    for r in (2, 1, 3):
        rcopy(s2.at[turn(x, r)], r2.at[r - 1], out_c, in_a, x_to(r), t).start()
        rcopy(sq2, rq2.at[r - 1], out_c, in_a, x_to(r), t).start()
    all_here(three(wo), wos, wor)
    s2b[...] = projection(lambda b: wo[b])
    for r in (2, 1, 3):
        rcopy(s2b.at[turn(x, r)], r2b.at[r - 1], out_c, in_b, x_to(r), t).start()
    state_in.wait()
    all_here(unit(42), out_c, in_a)

    sq = sq2[...]
    raw = s2[x].astype(f32)
    for i in range(N - 1):
        sq = sq + rq2[i]
        raw = raw + r2[i].astype(f32)
    lane = lax.broadcasted_iota(jnp.int32, (LOC, ROWS), 1)
    seq = lax.broadcasted_iota(jnp.int32, (LOC, ROWS), 0)
    total = jnp.sum(jnp.where(lane == seq + x * LOC, sq[0:1, :], 0.0), axis=1, keepdims=True)
    inv_a = lax.rsqrt(total / D + EPS)
    raw = raw * inv_a

    bound = lb_ref[...]
    forget_raw = raw[:, 128:256]
    forget = bound + (1.0 - bound) * sigmoid(forget_raw)
    keyvec = (1.0 - bound) * sigmoid(-forget_raw)
    query = silu(raw[:, 0:128])
    vals[...] = raw[:, 256:384]
    qfk[...] = jnp.concatenate([query * forget, forget, keyvec, jnp.zeros((LOC, 128), f32)], axis=0).T
    weight = jnp.sum(query * keyvec, axis=1, keepdims=True)

    for s in range(LOC):
        ho[s : s + 1, :] = jnp.sum(qfk[:, s : s + 1] * st[s], axis=0, keepdims=True)

    all_here(r2b, out_c, in_b)
    raw = s2b[x].astype(f32)
    for i in range(N - 1):
        raw = raw + r2b[i].astype(f32)
    out_gate = silu(raw * inv_a)
    head = ho[...] + weight * vals[...]
    inv = lax.rsqrt(jnp.mean(head * head, axis=1, keepdims=True) + EPS)
    n3[2 * x + c] = (head * inv * hg_ref[...] * out_gate).astype(bf16)

    mine3 = n3.at[2 * x + c]
    all_sent(unit(6), out_a, in_c)
    for r in (2, 1, 3):
        rcopy(mine3, mine3, out_a, in_c, x_to(r), mate).start()
        rcopy(mine3, mine3, out_a, in_c, x_to(r), t).start()
    rcopy(mine3, mine3, out_a, in_c, k, mate).start()
    all_here(three(wm.at[c]), wms, wmr)
    for b in range(N):
        rcopy(wm.at[c, b], wm.at[c, b], ms, mr, k, mate).start()
    for s in range(LOC):
        ns[s] = (
            qfk[:, LOC + s : LOC + s + 1] * st[s]
            + qfk[:, 2 * LOC + s : 2 * LOC + s + 1] * vals[s : s + 1, :]
        )
    all_here(wm.at[o], ms, mr)
    all_here(n3.at[pl.ds(0, 2 * N - 1)], out_a, in_c)

    heads = [jnp.concatenate([n3[4 * c + i], n3[4 * c + 2 + i]], axis=0) for i in range(2)]
    for b in range(N):
        mixed = jnp.dot(heads[0], wm[0, b], preferred_element_type=f32)
        mixed = mixed + jnp.dot(heads[1], wm[1, b], preferred_element_type=f32)
        for i in range(4):
            t4[4 * b + i] = mixed[16 * i : 16 * i + 16, :]
            s4[4 * b + i] = mixed[16 * i : 16 * i + 16, :].astype(bf16)

    def block_of(zz, cc):
        return (zz // 4) * 8 + cc * 4 + lax.rem(zz, 4)

    all_sent(x1.at[pl.ds(0, 2 * Z - 1)], out_b, in_c)
    for d in range(8, 0, -1):
        for r in ways(d):
            rcopy(s4.at[z_to(r)], r4.at[r - 1], out_b, r4s, k, 2 * z_to(r) + c).start()
    block = xf[z // 4, pl.ds(pl.multiple_of(c * 64 + lax.rem(z, 4) * 16, 16), 16), :] + t4[z]
    all_here(r4, out_b, r4s)
    for i in range(Z - 1):
        block = block + r4[i].astype(f32)
    own5[...] = block.astype(bf16)
    x5[block_of(z, c)] = own5[...]
    all_sent(unit(54), out_c, r4s)
    to_far(own5, x5, block_of, out_c)
    pass_to_mate(own5, x5, block_of, out_c)
    all_here(three(wgu), wgs, wgr)

    squares = jnp.zeros((ROWS, 1), f32)
    scaled = []
    for b in range(N):
        after = x5[8 * b : 8 * b + 8].reshape(ROWS, F).astype(f32)
        squares = squares + jnp.sum(after * after, axis=1, keepdims=True)
        scaled.append((after * gains[b, 1:2, :]).astype(bf16))

    def projected(i):
        acc = lax.dot_general(scaled[0], wgu[0, i], NT, preferred_element_type=f32)
        for b in range(1, N):
            acc = acc + lax.dot_general(scaled[b], wgu[b, i], NT, preferred_element_type=f32)
        return acc.astype(bf16).reshape(N, LOC, FFL)

    s6[:, 0, :, 0:FFL] = projected(0)
    s6[:, 1, :, 0:FFL] = projected(1)
    high = squares.astype(bf16).astype(f32)
    spot = lax.broadcasted_iota(jnp.int32, (ROWS, FFP - FFL), 1)
    tail = jnp.where(spot == 0, high, jnp.where(spot == 1, squares - high, 0.0))
    s6[:, 0, :, FFL:FFP] = tail.astype(bf16).reshape(N, LOC, FFP - FFL)
    s6[:, 1, :, FFL:FFP] = jnp.zeros((N, LOC, FFP - FFL), bf16)

    all_sent(unit(28), out_a, in_a)
    for r in (2, 1, 3):
        rcopy(s6.at[turn(x, r)], r6.at[r - 1], out_a, in_a, x_to(r), t).start()
    for b in range(N):
        xt5[b] = x5[8 * b : 8 * b + 8].reshape(ROWS, F).astype(f32).T.reshape(2 * Z, 8, ROWS)
    all_here(r6, out_a, in_a)
    gate = s6[x, 0].astype(f32)
    upper = s6[x, 1].astype(f32)
    for i in range(N - 1):
        gate = gate + r6[i, 0].astype(f32)
        upper = upper + r6[i, 1].astype(f32)
    total = gate[:, FFL : FFL + 1] + gate[:, FFL + 1 : FFL + 2]
    inverse = lax.rsqrt(total / D + EPS)
    hidden = silu(gate * inverse) * (upper * inverse)
    spot = lax.broadcasted_iota(jnp.int32, (LOC, FFP), 1)
    h7[x] = jnp.where(spot < FFL, hidden, 0.0).astype(bf16)

    all_sent(unit(60), out_b, in_b)
    for r in (2, 1, 3):
        rcopy(h7.at[x], h7.at[x], out_b, in_b, x_to(r), t).start()
    all_here(three(wd), wds, wdr)
    all_here(three(h7), out_b, in_b)
    hall = h7[...].reshape(ROWS, FFP)[:, 0:FFL]
    downs = [jnp.dot(hall, wd[b], preferred_element_type=f32).T for b in range(N)]
    swaps = []
    for b in range(N):
        for i in range(Z):
            even, odd = downs[b][16 * i : 16 * i + 8, :], downs[b][16 * i + 8 : 16 * i + 16, :]
            t8[i, b] = jnp.where(c == 0, even, odd)
            p8[b, i] = jnp.where(c == 0, odd, even).astype(bf16)
        swaps.append(rcopy(p8.at[b], d8.at[b], d8s, d8r.at[b], k, mate))
        swaps[b].start()

    all_sent(x5.at[pl.ds(0, 2 * Z - 1)], out_c, in_b)

    def piece(r, there):
        zz = z_to(r)
        rcopy(s8.at[zz, there], r8.at[y * Z + r], out_c, r8s, there * N + x, 2 * zz + c).start()

    t8[z] = t8[z] + xt5[:, t]
    for b in range(N):
        swaps[b].wait_recv()
        s8[:, b] = (t8[:, b] + d8[b].astype(f32)).astype(bf16)
        for d in range(8, 0, -1):
            for r in ways(d):
                piece(r, b)
    for q in range(1, N):
        piece(0, turn(y, q))
    r8[y * Z] = s8[z, y]
    all_here(unit(N * Z - 1), out_c, r8s)
    for b in range(N):
        acc = r8[b * Z].astype(f32)
        for i in range(1, Z):
            acc = acc + r8[b * Z + i].astype(f32)
        out_ref[:, ROWS * b : ROWS * b + ROWS] = acc.astype(bf16)

    for _, ref, ss, rs in weights:
        all_sent(three(ref), ss, rs)
    all_sent(wm.at[c], ms, mr)
    all_sent(unit(N * Z), d8s, r8s)
    all_sent(r6, out_a, in_a)
    all_sent(three(h7), out_b, in_b)
    all_sent(unit(N * Z - 1), out_c, r8s)


def write_out(out_ref, ns_ref, out_hbm, ns_hbm, sems):
    part = LOC // 4
    copies = [
        pltpu.make_async_copy(ns_ref.at[pl.ds(part * i, part)], ns_hbm.at[pl.ds(part * i, part)], sems.at[i])
        for i in range(4)
    ]
    copies.append(pltpu.make_async_copy(out_ref, out_hbm, sems.at[4]))
    for copy in copies:
        copy.start()
    for copy in copies:
        copy.wait()


def body(
    residual, mixer_gain, w_query, w_forget, w_input, w_outgate, lower_bound, state, head_gain,
    w_mix_out, ffn_gain, w_gate, w_up, w_down,
):
    vmem = pl.BlockSpec(memory_space=pltpu.VMEM)
    hbm = pl.BlockSpec(memory_space=pltpu.HBM)
    V = pltpu.VMEM
    dma = pltpu.SemaphoreType.DMA
    ring8 = [V((N, Z, 8, ROWS), bf16)] * 2 + [V((Z, N, 8, ROWS), bf16), V((N * Z, 8, ROWS), bf16)]
    scratch = [
        V((8, 4 * ROWS), bf16), V((1, F), f32), V((1, 128), f32), V((1, 128), f32), V((1, F), f32),
        V((N, 3, F, 128), bf16), V((N, F, 128), bf16), V((2, N, 128, F), bf16), V((N, 2, FFL, F), bf16), V((N, FFL, F), bf16),
        V((N, 2, F), f32), V((LOC, 128, 128), f32),
        V((N, 8, ROWS), bf16), V((2 * Z, N, 8, ROWS), bf16), V((N, ROWS, F), f32),
        V((N, LOC, 384), bf16), V((8, ROWS), f32), V((N - 1, LOC, 384), bf16), V((N - 1, 8, ROWS), f32),
        V((N, LOC, 128), bf16), V((N - 1, LOC, 128), bf16),
        V((128, 128), f32), V((LOC, 128), f32), V((LOC, 128), f32),
        V((2 * N, LOC, 128), bf16),
        V((Z, 16, F), f32), V((Z, 16, F), bf16), V((Z - 1, 16, F), bf16),
        V((16, F), bf16), V((2 * Z, 16, F), bf16), V((N, 2 * Z, 8, ROWS), f32),
        V((N, 2, LOC, FFP), bf16), V((N - 1, 2, LOC, FFP), bf16), V((N, LOC, FFP), bf16),
        V((Z, N, 8, ROWS), f32), *ring8,
        pltpu.SemaphoreType.REGULAR, dma((8,)), *([dma] * 17),
        dma, dma, dma, dma((8,)), *([dma] * 6), dma((N,)), dma,
    ]
    out, new_state = pl.pallas_call(
        layer_kernel,
        out_shape=(
            jax.ShapeDtypeStruct((8, 4 * ROWS), bf16),
            jax.ShapeDtypeStruct((LOC, 128, 128), f32),
        ),
        in_specs=[hbm] * 14,
        out_specs=(vmem, vmem),
        scratch_shapes=scratch,
        compiler_params=pltpu.CompilerParams(
            collective_id=0, has_side_effects=True, vmem_limit_bytes=24 * 1024 * 1024
        ),
    )(
        *(
            pltpu.with_memory_space_constraint(a, pltpu.HBM)
            for a in (
                residual.T, mixer_gain.reshape(1, F), lower_bound.reshape(1, 128), head_gain.reshape(1, 128),
                ffn_gain.reshape(1, F), w_query, w_forget, w_input, w_outgate, state.reshape(LOC, 128, 128),
                w_mix_out, w_gate.T, w_up.T, w_down,
            )
        ),
    )
    out, new_state = pl.pallas_call(
        write_out,
        out_shape=(
            jax.ShapeDtypeStruct((8, 4 * ROWS), bf16),
            jax.ShapeDtypeStruct((LOC, 128, 128), f32),
        ),
        in_specs=[vmem] * 2,
        out_specs=(hbm, hbm),
        scratch_shapes=[dma((5,))],
        compiler_params=pltpu.CompilerParams(vmem_limit_bytes=8 * 1024 * 1024),
    )(out, new_state)
    return out.T, new_state.reshape(LOC, 1, 128, 128)


def solution(mesh):
    in_specs = (
        P(None, ("kv", "tp")), P("kv"), P("kv", "tp"), P("kv", "tp"), P("kv", "tp"), P("kv", "tp"), P("tp"),
        P("kv", "tp", None, None), P(), P("tp", "kv"), P("kv"), P("kv", "tp"), P("kv", "tp"), P("tp", "kv"),
    )
    out_specs = (P(None, ("kv", "tp")), P("kv", "tp", None, None))
    return jax.shard_map(body, mesh=mesh, in_specs=in_specs, out_specs=out_specs, check_vma=False)
```

```python
import jax
import jax.numpy as jnp
from jax import lax
from jax.experimental import pallas as pl
from jax.experimental.pallas import tpu as pltpu
from jax.sharding import PartitionSpec as P

D = 4096
EPS = 1e-06
N = 4
Z = 16
ROWS = 128
LOC = 32
F = 256
FFL = 336
FFP = 384
MESH = pl.DeviceIdType.MESH
NT = (((1,), (1,)), ((), ()))
f32 = jnp.float32
bf16 = jnp.bfloat16


def sigmoid(u):
    return 1.0 / (1.0 + jnp.exp(-u))


def silu(u):
    return u * sigmoid(u)


def layer_kernel(
    x_hbm, mg_hbm, lb_hbm, hg_hbm, fg_hbm,
    wq_hbm, wf_hbm, wi_hbm, wo_hbm, state_hbm, wm_hbm, wg_hbm, wu_hbm, wd_hbm,
    out_ref, ns,
    x_ref, mg_ref, lb_ref, hg_ref, fg_ref, wp, wo, wm, wgu, wd, gains, st,
    xa, x1, xf, s2, sq2, r2, rq2, s2b, r2b, qfk, vals, ho, n3, t4, s4, r4, own5, x5, xt5,
    s6, r6, h7, t8, p8, d8, s8, r8,
    word, wsem, psem, gsem, stsem, wps, wpr, wos, wor, wms, wmr, wgs, wgr, wds, wdr, gr, r0, ms, mr,
    out_a, out_b, out_c, ring, fwd, in_a, in_b, in_c, r4s, d8s, d8r, r8s,
):
    k = lax.axis_index("kv")
    t = lax.axis_index("tp")
    z = t // 2
    c = lax.rem(t, 2)
    o = 1 - c
    y = k // N
    x = lax.rem(k, N)
    mate = 2 * z + o

    def turn(a, r):
        return lax.rem(a + r, N)

    def y_to(r):
        return turn(y, r) * N + x

    def x_to(r):
        return y * N + turn(x, r)

    def z_to(r):
        return lax.rem(z + r, Z)

    def z_from(r):
        return lax.rem(z - r + Z, Z)

    def rcopy(src, dst, ssem, rsem, kk, tt):
        return pltpu.make_async_remote_copy(
            src_ref=src, dst_ref=dst, send_sem=ssem, recv_sem=rsem,
            device_id=(kk, tt), device_id_type=MESH,
        )

    def all_sent(view, ssem, rsem):
        rcopy(view, view, ssem, rsem, k, mate).wait_send()

    def all_here(view, ssem, rsem):
        rcopy(view, view, ssem, rsem, k, mate).wait_recv()

    def unit(n):
        return r8.at[pl.ds(0, n)]

    def three(ref):
        return ref.at[pl.ds(0, N - 1)]

    def greet(kk, tt):
        barrier = pltpu.get_barrier_semaphore()
        pl.semaphore_signal(barrier, inc=1, device_id=(kk, tt), device_id_type=MESH)

    for d in range(4, 0, -1):
        greet(k, 2 * z_to(d) + c)
        greet(k, 2 * z_to(Z - d) + c)
    for r in (2, 1, 3):
        greet(y_to(r), t)
        greet(x_to(r), t)
    greet(k, mate)

    places = {
        "x": (x_hbm, x_ref), "mg": (mg_hbm, mg_ref), "fg": (fg_hbm, fg_ref),
        "o": (wo_hbm, wo.at[y]),
        "m": (wm_hbm, wm.at[c, y]), "d": (wd_hbm, wd.at[y]),
        "lb": (lb_hbm, lb_ref), "hg": (hg_hbm, hg_ref),
    }

    def pass_on(sem, d):
        for r in (d, Z - d):
            pl.semaphore_signal(sem, inc=1, device_id=(k, 2 * z_to(r) + c), device_id_type=MESH)

    loads = {
        name: pltpu.make_async_copy(src, dst, wsem.at[i]) for i, (name, (src, dst)) in enumerate(places.items())
    }
    for i, src in enumerate((wq_hbm, wf_hbm, wi_hbm)):
        pltpu.make_async_copy(src, wp.at[y, i], psem).start()
    for load in loads.values():
        load.start()
    for i, src in enumerate((wg_hbm, wu_hbm)):
        pltpu.make_async_copy(src, wgu.at[y, i], gsem).start()
    loads["p"] = pltpu.make_async_copy(wp.at[y], wp.at[y], psem)
    loads["g"] = pltpu.make_async_copy(wgu.at[y], wgu.at[y], gsem)
    loads["x"].wait()
    pl.semaphore_wait(pltpu.get_barrier_semaphore(), 8 + 2 * (N - 1) + 1)
    for r in (2, 1, 3):
        there = turn(y, r)
        lanes = pl.ds(pl.multiple_of(there * ROWS, ROWS), ROWS)
        rcopy(x_ref.at[:, lanes], xa.at[y], out_a, r0, y_to(r), t).start()
    pass_on(word, 4)
    loads["mg"].wait()
    loads["fg"].wait()
    gains[y, 0:1, :] = mg_ref[...]
    gains[y, 1:2, :] = fg_ref[...]
    for r in (2, 1, 3):
        rcopy(gains.at[y], gains.at[y], out_a, gr, y_to(r), t).start()
    weights = (
        ("p", wp, wps, wpr), ("o", wo, wos, wor), ("m", wm.at[c], wms, wmr), ("g", wgu, wgs, wgr), ("d", wd, wds, wdr),
    )

    def send_weights(name, ref, ss, rs):
        third = FFL // 3
        if name == "p":
            parts = [ref.at[y, i] for i in range(3)]
        elif name == "g":
            parts = [ref.at[y, i, pl.ds(third * j, third)] for i in range(2) for j in range(3)]
        elif name == "d":
            parts = [ref.at[y, pl.ds(third * j, third)] for j in range(3)]
        else:
            parts = [ref.at[y]]
        for part in parts:
            for r in (2, 1, 3):
                rcopy(part, part, ss, rs, y_to(r), t).start()

    for name, ref, ss, rs in weights:
        loads[name].wait()
        send_weights(name, ref, ss, rs)
    state_in = pltpu.make_async_copy(state_hbm, st, stsem)
    state_in.start()
    loads["lb"].wait()
    loads["hg"].wait()
    mine = pl.ds(pl.multiple_of(y * ROWS, ROWS), ROWS)
    xa[y] = x_ref[:, mine]
    all_here(three(xa), out_a, r0)

    def ways(d):
        return (d, Z - d) if d < 8 else (8,)

    def to_far(own, slots, slot, out):
        for d in range(8, 0, -1):
            for r in ways(d):
                rcopy(own, slots.at[slot(z, c)], out, ring.at[d - 1], k, 2 * z_to(r) + c).start()

    def pass_to_mate(own, slots, slot, out):
        rcopy(own, slots.at[slot(z, c)], out, fwd, k, mate).start()
        for d in range(1, 9):
            all_here(slots.at[pl.ds(0, len(ways(d)))], out, ring.at[d - 1])
            for r in ways(d):
                src = slots.at[slot(z_from(r), c)]
                rcopy(src, src, out, fwd, k, mate).start()
        all_here(slots.at[pl.ds(0, Z)], out, fwd)

    x1[t] = xa[...]

    def by_tp(zz, cc):
        return 2 * zz + cc

    pl.semaphore_wait(word, 2)
    to_far(xa, x1, by_tp, out_b)
    pass_to_mate(xa, x1, by_tp, out_b)
    all_here(three(gains), out_a, gr)
    all_here(three(wp), wps, wpr)

    row = jnp.zeros((1, ROWS), f32)
    scaled = []
    for b in range(N):
        xt = x1[:, b].astype(f32).reshape(F, ROWS)
        row = row + jnp.sum(xt * xt, axis=0, keepdims=True)
        rows = xt.T
        xf[b] = rows
        scaled.append((rows * gains[b, 0:1, :]).astype(bf16))
    sq2[...] = jnp.broadcast_to(row, (8, ROWS))

    def projection(w):
        part = jnp.dot(scaled[0], w(0), preferred_element_type=f32)
        for b in range(1, N):
            part = part + jnp.dot(scaled[b], w(b), preferred_element_type=f32)
        return part.astype(bf16).reshape(N, LOC, 128)

    for i in range(3):
        s2[:, :, 128 * i : 128 * i + 128] = projection(lambda b, i=i: wp[b, i])

    for r in (2, 1, 3):
        rcopy(s2.at[turn(x, r)], r2.at[r - 1], out_c, in_a, x_to(r), t).start()
        rcopy(sq2, rq2.at[r - 1], out_c, in_a, x_to(r), t).start()
    all_here(three(wo), wos, wor)
    s2b[...] = projection(lambda b: wo[b])
    for r in (2, 1, 3):
        rcopy(s2b.at[turn(x, r)], r2b.at[r - 1], out_c, in_b, x_to(r), t).start()
    state_in.wait()
    all_here(unit(42), out_c, in_a)

    sq = sq2[...]
    raw = s2[x].astype(f32)
    for i in range(N - 1):
        sq = sq + rq2[i]
        raw = raw + r2[i].astype(f32)
    lane = lax.broadcasted_iota(jnp.int32, (LOC, ROWS), 1)
    seq = lax.broadcasted_iota(jnp.int32, (LOC, ROWS), 0)
    total = jnp.sum(jnp.where(lane == seq + x * LOC, sq[0:1, :], 0.0), axis=1, keepdims=True)
    inv_a = lax.rsqrt(total / D + EPS)
    raw = raw * inv_a

    bound = lb_ref[...]
    forget_raw = raw[:, 128:256]
    forget = bound + (1.0 - bound) * sigmoid(forget_raw)
    keyvec = (1.0 - bound) * sigmoid(-forget_raw)
    query = silu(raw[:, 0:128])
    vals[...] = raw[:, 256:384]
    qfk[...] = jnp.concatenate([query * forget, forget, keyvec, jnp.zeros((LOC, 128), f32)], axis=0).T
    weight = jnp.sum(query * keyvec, axis=1, keepdims=True)

    for s in range(LOC):
        ho[s : s + 1, :] = jnp.sum(qfk[:, s : s + 1] * st[s], axis=0, keepdims=True)

    all_here(r2b, out_c, in_b)
    raw = s2b[x].astype(f32)
    for i in range(N - 1):
        raw = raw + r2b[i].astype(f32)
    out_gate = silu(raw * inv_a)
    head = ho[...] + weight * vals[...]
    inv = lax.rsqrt(jnp.mean(head * head, axis=1, keepdims=True) + EPS)
    n3[2 * x + c] = (head * inv * hg_ref[...] * out_gate).astype(bf16)

    mine3 = n3.at[2 * x + c]
    all_sent(unit(6), out_a, in_c)
    for r in (2, 1, 3):
        rcopy(mine3, mine3, out_a, in_c, x_to(r), t).start()
        rcopy(mine3, mine3, out_a, in_c, x_to(r), mate).start()
    rcopy(mine3, mine3, out_a, in_c, k, mate).start()
    all_here(three(wm.at[c]), wms, wmr)
    rcopy(wm.at[c], wm.at[c], ms, mr, k, mate).start()
    for s in range(LOC):
        ns[s] = (
            qfk[:, LOC + s : LOC + s + 1] * st[s]
            + qfk[:, 2 * LOC + s : 2 * LOC + s + 1] * vals[s : s + 1, :]
        )
    all_here(wm.at[o], ms, mr)
    all_here(n3.at[pl.ds(0, 2 * N - 1)], out_a, in_c)

    heads = [jnp.concatenate([n3[4 * c + i], n3[4 * c + 2 + i]], axis=0) for i in range(2)]
    for b in range(N):
        mixed = jnp.dot(heads[0], wm[0, b], preferred_element_type=f32)
        mixed = mixed + jnp.dot(heads[1], wm[1, b], preferred_element_type=f32)
        for i in range(4):
            t4[4 * b + i] = mixed[16 * i : 16 * i + 16, :]
            s4[4 * b + i] = mixed[16 * i : 16 * i + 16, :].astype(bf16)

    def block_of(zz, cc):
        return (zz // 4) * 8 + cc * 4 + lax.rem(zz, 4)

    all_sent(x1.at[pl.ds(0, 2 * Z - 1)], out_b, in_c)
    for d in range(8, 0, -1):
        for r in ways(d):
            rcopy(s4.at[z_to(r)], r4.at[r - 1], out_b, r4s, k, 2 * z_to(r) + c).start()
    block = xf[z // 4, pl.ds(pl.multiple_of(c * 64 + lax.rem(z, 4) * 16, 16), 16), :] + t4[z]
    all_here(r4, out_b, r4s)
    for i in range(Z - 1):
        block = block + r4[i].astype(f32)
    own5[...] = block.astype(bf16)
    x5[block_of(z, c)] = own5[...]
    all_sent(unit(54), out_c, r4s)
    to_far(own5, x5, block_of, out_c)
    pass_to_mate(own5, x5, block_of, out_c)
    all_here(three(wgu), wgs, wgr)

    squares = jnp.zeros((ROWS, 1), f32)
    scaled = []
    for b in range(N):
        after = x5[8 * b : 8 * b + 8].reshape(ROWS, F).astype(f32)
        squares = squares + jnp.sum(after * after, axis=1, keepdims=True)
        scaled.append((after * gains[b, 1:2, :]).astype(bf16))

    def projected(i):
        acc = lax.dot_general(scaled[0], wgu[0, i], NT, preferred_element_type=f32)
        for b in range(1, N):
            acc = acc + lax.dot_general(scaled[b], wgu[b, i], NT, preferred_element_type=f32)
        return acc.astype(bf16).reshape(N, LOC, FFL)

    s6[:, 0, :, 0:FFL] = projected(0)
    s6[:, 1, :, 0:FFL] = projected(1)
    high = squares.astype(bf16).astype(f32)
    spot = lax.broadcasted_iota(jnp.int32, (ROWS, FFP - FFL), 1)
    tail = jnp.where(spot == 0, high, jnp.where(spot == 1, squares - high, 0.0))
    s6[:, 0, :, FFL:FFP] = tail.astype(bf16).reshape(N, LOC, FFP - FFL)
    s6[:, 1, :, FFL:FFP] = jnp.zeros((N, LOC, FFP - FFL), bf16)

    all_sent(unit(28), out_a, in_a)
    for r in (2, 1, 3):
        rcopy(s6.at[turn(x, r)], r6.at[r - 1], out_a, in_a, x_to(r), t).start()
    for b in range(N):
        xt5[b] = x5[8 * b : 8 * b + 8].reshape(ROWS, F).astype(f32).T.reshape(2 * Z, 8, ROWS)
    all_here(r6, out_a, in_a)
    gate = s6[x, 0].astype(f32)
    upper = s6[x, 1].astype(f32)
    for i in range(N - 1):
        gate = gate + r6[i, 0].astype(f32)
        upper = upper + r6[i, 1].astype(f32)
    total = gate[:, FFL : FFL + 1] + gate[:, FFL + 1 : FFL + 2]
    inverse = lax.rsqrt(total / D + EPS)
    hidden = silu(gate * inverse) * (upper * inverse)
    spot = lax.broadcasted_iota(jnp.int32, (LOC, FFP), 1)
    h7[x] = jnp.where(spot < FFL, hidden, 0.0).astype(bf16)

    all_sent(unit(60), out_b, in_b)
    for r in (2, 1, 3):
        rcopy(h7.at[x], h7.at[x], out_b, in_b, x_to(r), t).start()
    all_here(three(wd), wds, wdr)
    all_here(three(h7), out_b, in_b)
    hall = h7[...].reshape(ROWS, FFP)[:, 0:FFL]
    downs = [jnp.dot(hall, wd[b], preferred_element_type=f32).T for b in range(N)]
    swaps = []
    for b in range(N):
        for i in range(Z):
            even, odd = downs[b][16 * i : 16 * i + 8, :], downs[b][16 * i + 8 : 16 * i + 16, :]
            t8[i, b] = jnp.where(c == 0, even, odd)
            p8[b, i] = jnp.where(c == 0, odd, even).astype(bf16)
        swaps.append(rcopy(p8.at[b], d8.at[b], d8s, d8r.at[b], k, mate))
        swaps[b].start()

    all_sent(x5.at[pl.ds(0, 2 * Z - 1)], out_c, in_b)

    def piece(r, there):
        zz = z_to(r)
        rcopy(s8.at[zz, there], r8.at[y * Z + r], out_c, r8s, there * N + x, 2 * zz + c).start()

    t8[z] = t8[z] + xt5[:, t]
    for b in range(N):
        swaps[b].wait_recv()
        s8[:, b] = (t8[:, b] + d8[b].astype(f32)).astype(bf16)
        for d in range(8, 0, -1):
            for r in ways(d):
                piece(r, b)
    for q in range(1, N):
        piece(0, turn(y, q))
    r8[y * Z] = s8[z, y]
    all_here(unit(N * Z - 1), out_c, r8s)
    for b in range(N):
        acc = r8[b * Z].astype(f32)
        for i in range(1, Z):
            acc = acc + r8[b * Z + i].astype(f32)
        out_ref[:, ROWS * b : ROWS * b + ROWS] = acc.astype(bf16)

    for _, ref, ss, rs in weights:
        all_sent(three(ref), ss, rs)
    all_sent(wm.at[c], ms, mr)
    all_sent(unit(N * Z), d8s, r8s)
    all_sent(r6, out_a, in_a)
    all_sent(three(h7), out_b, in_b)
    all_sent(unit(N * Z - 1), out_c, r8s)


def write_out(out_ref, ns_ref, out_hbm, ns_hbm, sems):
    part = LOC // 4
    copies = [
        pltpu.make_async_copy(ns_ref.at[pl.ds(part * i, part)], ns_hbm.at[pl.ds(part * i, part)], sems.at[i])
        for i in range(4)
    ]
    copies.append(pltpu.make_async_copy(out_ref, out_hbm, sems.at[4]))
    for copy in copies:
        copy.start()
    for copy in copies:
        copy.wait()


def body(
    residual, mixer_gain, w_query, w_forget, w_input, w_outgate, lower_bound, state, head_gain,
    w_mix_out, ffn_gain, w_gate, w_up, w_down,
):
    vmem = pl.BlockSpec(memory_space=pltpu.VMEM)
    hbm = pl.BlockSpec(memory_space=pltpu.HBM)
    V = pltpu.VMEM
    dma = pltpu.SemaphoreType.DMA
    ring8 = [V((N, Z, 8, ROWS), bf16)] * 2 + [V((Z, N, 8, ROWS), bf16), V((N * Z, 8, ROWS), bf16)]
    scratch = [
        V((8, 4 * ROWS), bf16), V((1, F), f32), V((1, 128), f32), V((1, 128), f32), V((1, F), f32),
        V((N, 3, F, 128), bf16), V((N, F, 128), bf16), V((2, N, 128, F), bf16), V((N, 2, FFL, F), bf16), V((N, FFL, F), bf16),
        V((N, 2, F), f32), V((LOC, 128, 128), f32),
        V((N, 8, ROWS), bf16), V((2 * Z, N, 8, ROWS), bf16), V((N, ROWS, F), f32),
        V((N, LOC, 384), bf16), V((8, ROWS), f32), V((N - 1, LOC, 384), bf16), V((N - 1, 8, ROWS), f32),
        V((N, LOC, 128), bf16), V((N - 1, LOC, 128), bf16),
        V((128, 128), f32), V((LOC, 128), f32), V((LOC, 128), f32),
        V((2 * N, LOC, 128), bf16),
        V((Z, 16, F), f32), V((Z, 16, F), bf16), V((Z - 1, 16, F), bf16),
        V((16, F), bf16), V((2 * Z, 16, F), bf16), V((N, 2 * Z, 8, ROWS), f32),
        V((N, 2, LOC, FFP), bf16), V((N - 1, 2, LOC, FFP), bf16), V((N, LOC, FFP), bf16),
        V((Z, N, 8, ROWS), f32), *ring8,
        pltpu.SemaphoreType.REGULAR, dma((8,)), *([dma] * 17),
        dma, dma, dma, dma((8,)), *([dma] * 6), dma((N,)), dma,
    ]
    out, new_state = pl.pallas_call(
        layer_kernel,
        out_shape=(
            jax.ShapeDtypeStruct((8, 4 * ROWS), bf16),
            jax.ShapeDtypeStruct((LOC, 128, 128), f32),
        ),
        in_specs=[hbm] * 14,
        out_specs=(vmem, vmem),
        scratch_shapes=scratch,
        compiler_params=pltpu.CompilerParams(
            collective_id=0, has_side_effects=True, vmem_limit_bytes=24 * 1024 * 1024
        ),
    )(
        *(
            pltpu.with_memory_space_constraint(a, pltpu.HBM)
            for a in (
                residual.T, mixer_gain.reshape(1, F), lower_bound.reshape(1, 128), head_gain.reshape(1, 128),
                ffn_gain.reshape(1, F), w_query, w_forget, w_input, w_outgate, state.reshape(LOC, 128, 128),
                w_mix_out, w_gate.T, w_up.T, w_down,
            )
        ),
    )
    out, new_state = pl.pallas_call(
        write_out,
        out_shape=(
            jax.ShapeDtypeStruct((8, 4 * ROWS), bf16),
            jax.ShapeDtypeStruct((LOC, 128, 128), f32),
        ),
        in_specs=[vmem] * 2,
        out_specs=(hbm, hbm),
        scratch_shapes=[dma((5,))],
        compiler_params=pltpu.CompilerParams(vmem_limit_bytes=8 * 1024 * 1024),
    )(out, new_state)
    return out.T, new_state.reshape(LOC, 1, 128, 128)


def solution(mesh):
    in_specs = (
        P(None, ("kv", "tp")), P("kv"), P("kv", "tp"), P("kv", "tp"), P("kv", "tp"), P("kv", "tp"), P("tp"),
        P("kv", "tp", None, None), P(), P("tp", "kv"), P("kv"), P("kv", "tp"), P("kv", "tp"), P("tp", "kv"),
    )
    out_specs = (P(None, ("kv", "tp")), P("kv", "tp", None, None))
    return jax.shard_map(body, mesh=mesh, in_specs=in_specs, out_specs=out_specs, check_vma=False)
```
